256 devices in a mesh: sp: 64 (over z, x, core), tp: 4 (over y).
Axes of the slice: x: 4, y: 4, z: 8, core: 2. Of those that a mesh axis runs over, the one named last changes fastest.
Arguments:
- conv_value: bfloat16 [32768, 1024], P('sp', 'tp'), may hold values from -6 to 6
- conv_gate: bfloat16 [32768, 1024], P('sp', 'tp'), may hold values from -9 to 9
- conv_weight: float32 [31, 1024], P(None, 'tp'), may hold values from -2.2 to 2.2
- conv_gain: float32 [1024], P('tp'), may hold values from 0.1 to 1.9
- conv_shift: float32 [1024], P('tp'), may hold values from -3 to 3
- out_weight: bfloat16 [1024, 2048], P('tp'), may hold values from -0.1875 to 0.1875
- residual: bfloat16 [32768, 2048], P('sp', 'tp'), may hold values from -10 to 10
- mix_gain: float32 [2048], P('tp'), may hold values from 0.1 to 1.9
- expert_ids: int32 [32768, 2], P('sp'), may hold values from 0 to 63, all different within a row; in each aligned block of 128 rows (0 to 127, 128 to 255, ...) at most 8 rows name the same one
- group_weight: float32 [32768], P('sp'), may hold values from 0.6 to 1
- score_gap: float32 [32768], P('sp'), may hold values from -0.8 to 0.8
- w_gate: bfloat16 [64, 2048, 1024], P('sp', None, 'tp'), may hold values from -0.125 to 0.125
- w_up: bfloat16 [64, 2048, 1024], P('sp', None, 'tp'), may hold values from -0.125 to 0.125
- w_down: bfloat16 [64, 1024, 2048], P('sp', 'tp'), may hold values from -0.1875 to 0.1875
Outputs:
- layer_out: bfloat16 [32768, 2048], P('sp', 'tp')
The draws below stay inside these ranges and needn't reach their ends.
Inputs may be any that keep to these rules, and one draw needn't show every extreme that they name: `expert_ids`: the two experts of a position differ. In each aligned block of 512 // 4 positions no expert is named by more than 8 rows, a bound that some block reaches.
All inputs are finite; a program needn't handle non-finite values.
Results may differ from the reference program's by a relative error of at most 0.012.
Values may be sent and summed in bfloat16 or wider, within the bound.
A program may use at most 128 MiB of HBM per device.

```python
import math
import jax
import jax.numpy as jnp
import numpy as np
from jax import lax

D = 2048
CH = 1024
FF = 1024
KW = 31
ROWS = 512
TOKENS = 32768
EXPERTS = 64
CAP = 8
N_SP = 64
N_TP = 4


def draw_conv_weight(key, part):
    rising = jnp.exp(jnp.linspace(math.log(0.3), math.log(3.0), CH)).astype(jnp.float32)
    base = jnp.clip(jax.random.normal(key, (KW, CH), jnp.float32), -4.0, 4.0)
    return (base * rising[None, :] / math.sqrt(KW)).astype(jnp.float32)


def draw_residual(key, part):
    rising = jnp.exp(jnp.linspace(math.log(0.5), math.log(2.0), D)).astype(jnp.float32)
    base = jnp.clip(jax.random.normal(key, (TOKENS, D), jnp.float32), -5.0, 5.0)
    return (base * rising[None, :]).astype(jnp.bfloat16)


def levels(key, extent, shards, smallest, high):
    def one(axis_at, blocks):
        steps = jax.random.uniform(jax.random.fold_in(jax.random.fold_in(key, 6), axis_at), (blocks,), jnp.float32, smallest / len(shards), high / len(shards))
        return jnp.repeat(jnp.exp(steps), extent[axis_at] // blocks).reshape((-1,) + (1,) * (len(extent) - axis_at - 1))

    level = one(*shards[0])
    for cut in shards[1:]:
        level = level * one(*cut)
    return level


def assign_block(stream_key, own, number, rows, amount, top, bound, lean):
    sequence = jax.random.permutation(stream_key, amount)
    heavy_load, common = load_shares(amount, rows * top, bound, lean, True), load_shares(amount, rows * top, bound, lean, False)
    places = jnp.arange(amount)

    def named(tallies, offset_by):
        used = int((tallies > 0).sum())
        fixed = max(1, used // 4)
        passed = fixed + (places - fixed + offset_by * (used - fixed)) % max(1, amount - fixed)
        return jnp.zeros((amount,), jnp.int32).at[sequence[jnp.where(places < fixed, places, passed)]].set(jnp.asarray(tallies, jnp.int32))

    tallies = jnp.where(number % 4 == 0, named(heavy_load, number // 4), named(common, number - number // 4 - 1))
    mixed = jax.random.permutation(jax.random.fold_in(own, 3), amount)
    donor, receiver = mixed[0:amount // 2 * 2:2], mixed[1:amount // 2 * 2:2]
    margin = jnp.minimum(tallies[donor] - 1, bound - tallies[receiver]) // 2
    margin = jnp.where((donor == sequence[0]) | (receiver == sequence[0]) | (tallies[receiver] == 0), 0, jnp.maximum(margin, 0))
    passed = jax.random.randint(jax.random.fold_in(own, 4), (amount // 2,), 0, 1 << 20) % (margin + 1)
    tallies = tallies.at[donor].add(-passed).at[receiver].add(passed)
    items = jnp.searchsorted(jnp.cumsum(tallies), jnp.arange(rows * top), side="right").astype(jnp.int32)
    grid = items.reshape(top, rows).T
    grid = grid[jax.random.permutation(jax.random.fold_in(own, 1), rows)]
    offset_by = jax.random.randint(jax.random.fold_in(own, 2), (rows, 1), 0, top)
    return jnp.take_along_axis(grid, (jnp.arange(top)[None, :] + offset_by) % top, axis=1)


def load_shares(count, total, most, skew, full):
    loads = [(1 << 20) // math.isqrt(standing ** skew) + 1 for standing in range(1, count + 1)]
    largest = most if full else min(most, max(-(-total // count), total * loads[0] // sum(loads)))
    least = 1 if total - largest >= count - 1 else 0
    holding, surplus = [largest] + [least] * (count - 1), total - largest - least * (count - 1)
    while surplus > 0:
        candidates = [i for i in range(1, count) if holding[i] < largest] or [i for i in range(1, count) if holding[i] < most]
        pool, left = sum([loads[i] for i in candidates]), surplus
        for i in candidates:
            extra = min(most - holding[i], max(1, left * loads[i] // pool), surplus)
            holding[i] = holding[i] + extra
            surplus = surplus - extra
    return np.array(holding)


def scatter_about(own_key, shape, spread, reach, split=(), kind=jnp.bfloat16):
    entries = jax.random.normal(own_key, shape, jnp.float32) * spread
    if len(split) > 0:
        entries = levels(own_key, shape, split, -0.22, 0.18) * entries
    return jnp.clip(entries, min=-reach, max=reach).astype(kind)


def setup_inputs(seed: int = 0) -> dict:
    splits = jax.random.split(jax.random.key(seed), 15)
    conv_value = scatter_about(splits[0], (TOKENS, CH), 1.0, 6.0, ((0, 64), (1, 4)))
    conv_gate = scatter_about(splits[1], (TOKENS, CH), 1.5, 9.0, ((0, 64), (1, 4)))
    conv_weight = draw_conv_weight(jax.random.fold_in(splits[14], 71), 0)
    conv_gain = jnp.clip(1.0 + 0.18 * jax.random.normal(splits[3], (CH,), jnp.float32), 0.1, 1.9)
    conv_shift = scatter_about(splits[4], (CH,), 0.5, 3.0, ((0, 4),), jnp.float32)
    out_weight = scatter_about(splits[5], (CH, D), CH ** -0.5, 0.1875, ((0, 4),))
    residual = draw_residual(jax.random.fold_in(splits[14], 71), 0)
    mix_gain = jnp.clip(1.0 + 0.18 * jax.random.normal(splits[7], (D,), jnp.float32), 0.1, 1.9)
    expert_ids_keys = jax.random.split(jax.random.fold_in(splits[8], 1), TOKENS // (ROWS // N_TP))
    expert_ids_turns = jax.random.permutation(jax.random.fold_in(splits[8], 3), TOKENS // (ROWS // N_TP))
    expert_ids = jax.vmap(lambda own, number: assign_block(jax.random.fold_in(splits[8], 2), own, number, ROWS // N_TP, EXPERTS, 2, CAP, 2))(expert_ids_keys, expert_ids_turns).reshape((TOKENS, 2))
    group_weight = jnp.clip(0.6 + 0.39999998 * jax.random.uniform(splits[9], (TOKENS,), jnp.float32) ** levels(splits[9], (TOKENS,), ((0, 64),), -0.2, 0.2), 0.6, 1.0)
    score_gap = jnp.clip(jax.random.uniform(splits[10], (TOKENS,), jnp.float32, -0.8, 0.8) * levels(splits[10], (TOKENS,), ((0, 64),), -0.4, 0.0), -0.8, 0.8)
    w_gate = scatter_about(splits[11], (EXPERTS, D, FF), D ** -0.5, 0.125, ((0, 64), (2, 4)))
    w_up = scatter_about(splits[12], (EXPERTS, D, FF), D ** -0.5, 0.125, ((0, 64), (2, 4)))
    w_down = scatter_about(splits[13], (EXPERTS, FF, D), FF ** -0.5, 0.1875, ((0, 64), (1, 4)))
    return {"conv_value": conv_value, "conv_gate": conv_gate, "conv_weight": conv_weight, "conv_gain": conv_gain, "conv_shift": conv_shift, "out_weight": out_weight, "residual": residual, "mix_gain": mix_gain, "expert_ids": expert_ids, "group_weight": group_weight, "score_gap": score_gap, "w_gate": w_gate, "w_up": w_up, "w_down": w_down}


eps = 1e-06

def reference(conv_value, conv_gate, conv_weight, conv_gain, conv_shift, out_weight, residual, mix_gain, expert_ids, group_weight, score_gap, w_gate, w_up, w_down):
    gated = conv_value.astype(jnp.float32) * jax.nn.sigmoid(conv_gate.astype(jnp.float32))
    padded = jnp.pad(gated, ((KW - 1, 0), (0, 0)))
    convolved = jnp.zeros_like(gated)
    for tap_index in range(KW):
        convolved = convolved + conv_weight[tap_index] * padded[tap_index:tap_index + TOKENS]
    row_mean = lax.optimization_barrier(jnp.mean(convolved, axis=-1, keepdims=True))
    row_var = lax.optimization_barrier(jnp.mean(convolved * convolved, axis=-1, keepdims=True)) - row_mean * row_mean
    normalized = (convolved - row_mean) * lax.rsqrt(row_var + eps) * conv_gain + conv_shift
    activated = jax.nn.silu(normalized).astype(jnp.bfloat16)
    block_width = CH // N_TP
    mixed = jnp.zeros((TOKENS, D), jnp.float32)
    for block_index in range(N_TP):
        low = block_index * block_width
        term = jnp.dot(activated[:, low:low + block_width], out_weight[low:low + block_width], preferred_element_type=jnp.float32)
        mixed = mixed + term.astype(jnp.bfloat16).astype(jnp.float32)
    middle = (residual.astype(jnp.float32) + mixed).astype(jnp.bfloat16)
    middle_wide = middle.astype(jnp.float32)
    normed = (middle_wide * lax.rsqrt(lax.optimization_barrier(jnp.mean(middle_wide * middle_wide, axis=-1, keepdims=True)) + eps) * mix_gain).astype(jnp.bfloat16)
    assign_count = TOKENS * 2
    expert_cap = N_SP * N_TP * CAP
    flat_experts = expert_ids.reshape(-1)
    token_of = jnp.concatenate([jnp.arange(assign_count, dtype=jnp.int32) // 2, jnp.array([TOKENS], jnp.int32)])
    normed_pad = jnp.concatenate([normed, jnp.zeros((1, D), jnp.bfloat16)], axis=0).astype(jnp.float32)
    hidden_width = FF // N_TP

    def expert_step(carry, expert):
        positions = jnp.nonzero(flat_experts == expert, size=expert_cap, fill_value=assign_count)[0].astype(jnp.int32)
        chosen = normed_pad[token_of[positions]]
        gate_part = jnp.dot(chosen, w_gate[expert].astype(jnp.float32))
        up_part = jnp.dot(chosen, w_up[expert].astype(jnp.float32))
        hidden = (jax.nn.silu(gate_part) * up_part).astype(jnp.bfloat16).astype(jnp.float32)
        down = w_down[expert].astype(jnp.float32)
        total = jnp.zeros((expert_cap, D), jnp.float32)
        for block_index in range(N_TP):
            low = block_index * hidden_width
            term = jnp.dot(hidden[:, low:low + hidden_width], down[low:low + hidden_width])
            total = total + term.astype(jnp.bfloat16).astype(jnp.float32)
        carry = carry.at[positions].set(total.astype(jnp.bfloat16))
        return (carry, None)
    start = jnp.zeros((assign_count + 1, D), jnp.bfloat16)
    results, _ = lax.scan(expert_step, start, jnp.arange(EXPERTS, dtype=jnp.int32))
    picked = results[:assign_count].reshape(TOKENS, 2, D).astype(jnp.float32)
    first_gate = group_weight * jax.nn.sigmoid(score_gap)
    second_gate = group_weight * jax.nn.sigmoid(-score_gap)
    layer_out = middle_wide + first_gate[:, None] * picked[:, 0] + second_gate[:, None] * picked[:, 1]
    return layer_out.astype(jnp.bfloat16)
```

```python
import jax
import jax.numpy as jnp
from jax import lax
from jax.sharding import PartitionSpec as P

D = 2048
CH = 1024


eps = 1e-06


def passed_along(value, axis, steps):
    count = lax.axis_size(axis)
    leading, last = (max(0, -steps), min(count, count - steps))
    return lax.ppermute(value, axis, [(source, source + steps) for source in range(leading, last)])


def from_everyone(shard, axis):
    copies = jnp.broadcast_to(shard, (lax.axis_size(axis), *shard.shape))
    return lax.all_to_all(copies, axis, split_axis=0, concat_axis=0, tiled=True)


def shards(
    conv_value,
    conv_gate,
    conv_weight,
    conv_gain,
    conv_shift,
    out_weight,
    residual,
    mix_gain,
    expert_ids,
    group_weight,
    score_gap,
    w_gate,
    w_up,
    w_down,
):
    row_count = conv_value.shape[0]
    reach_rows = conv_weight.shape[0] - 1
    sp = lax.axis_size("sp")
    tp = lax.axis_size("tp")
    quarter = row_count // tp
    capacity = 4 * quarter // sp
    me = lax.axis_index("tp")
    out_full = lax.all_gather(out_weight, "tp", axis=0, tiled=False)
    gate_full = lax.all_gather(w_gate[0], "tp", axis=0, tiled=False)
    up_full = lax.all_gather(w_up[0], "tp", axis=0, tiled=False)
    down_full = lax.all_gather(w_down[0], "tp", axis=0, tiled=False)
    gain_full = from_everyone(mix_gain[None], "tp").reshape(-1)
    residual_q = lax.all_to_all(residual, "tp", split_axis=0, concat_axis=1, tiled=True)

    prev_value, prev_gate = passed_along(
        (conv_value[row_count - reach_rows :], conv_gate[row_count - reach_rows :]), "sp", 1
    )
    values = jnp.concatenate([prev_value, conv_value], axis=0).astype(jnp.float32)
    gate_pre = jnp.concatenate([prev_gate, conv_gate], axis=0).astype(jnp.float32)
    gated = values * jax.nn.sigmoid(gate_pre)
    convolved = jnp.zeros((row_count, conv_value.shape[1]), jnp.float32)
    for tap_index in range(reach_rows + 1):
        convolved = convolved + conv_weight[tap_index] * gated[tap_index : tap_index + row_count]
    stats = jnp.stack([jnp.sum(convolved, axis=-1), jnp.sum(convolved * convolved, axis=-1)])
    stats = jnp.sum(from_everyone(stats.reshape(1, -1), "tp"), axis=0).reshape(2, -1)
    row_mean = (stats[0] / CH)[:, None]
    row_var = (stats[1] / CH)[:, None] - row_mean * row_mean
    normalized = (convolved - row_mean) * lax.rsqrt(row_var + eps) * conv_gain + conv_shift
    activated = jax.nn.silu(normalized).astype(jnp.bfloat16)
    act_q = lax.all_to_all(activated.reshape(tp, quarter, -1), "tp", 0, 0, tiled=True)
    middle_wide = residual_q.astype(jnp.float32)
    mixed = jnp.zeros((quarter, D), jnp.float32)
    for b in range(tp):
        term = jnp.dot(act_q[b], out_full[b], preferred_element_type=jnp.float32)
        mixed = mixed + term.astype(jnp.bfloat16).astype(jnp.float32)
    middle = (middle_wide + mixed).astype(jnp.bfloat16)
    middle_wide = middle.astype(jnp.float32)
    row_sq = jnp.mean(middle_wide * middle_wide, axis=-1, keepdims=True)
    normed = (middle_wide * lax.rsqrt(row_sq + eps) * gain_full).astype(jnp.bfloat16)
    ids = lax.dynamic_slice_in_dim(expert_ids, me * quarter, quarter, 0)
    gw = lax.dynamic_slice_in_dim(group_weight, me * quarter, quarter, 0)
    gap = lax.dynamic_slice_in_dim(score_gap, me * quarter, quarter, 0)
    experts = jnp.arange(sp, dtype=jnp.int32)
    hit = [(ids[:, k : k + 1] == experts[None]).astype(jnp.bfloat16) for k in range(2)]
    both = hit[0] + hit[1]
    rows = jnp.arange(quarter)
    lower = (rows[None, :] < rows[:, None]).astype(jnp.bfloat16)
    before = jnp.dot(lower, both, preferred_element_type=jnp.float32)
    slots = jnp.arange(sp * capacity, dtype=jnp.int32)
    places = []
    for k in range(2):
        rank = jnp.sum(before * hit[k].astype(jnp.float32), axis=1).astype(jnp.int32)
        slot = ids[:, k] * capacity + rank
        places.append((slot[:, None] == slots[None, :]).astype(jnp.bfloat16))
    send = (places[0] + places[1]).T
    outgoing = jnp.dot(send, normed, preferred_element_type=jnp.float32).astype(jnp.bfloat16)
    received = lax.all_to_all(
        outgoing.reshape(sp, capacity, D), "sp", split_axis=0, concat_axis=0, tiled=True
    ).reshape(-1, D)
    total = jnp.zeros((sp * capacity, D), jnp.float32)
    for b in range(tp):
        g = jnp.dot(received, gate_full[b], preferred_element_type=jnp.float32)
        u = jnp.dot(received, up_full[b], preferred_element_type=jnp.float32)
        hidden = (jax.nn.silu(g) * u).astype(jnp.bfloat16)
        term = jnp.dot(hidden, down_full[b], preferred_element_type=jnp.float32)
        total = total + term.astype(jnp.bfloat16).astype(jnp.float32)
    returned = lax.all_to_all(
        total.astype(jnp.bfloat16).reshape(sp, capacity, D), "sp", 0, 0, tiled=True
    ).reshape(-1, D)
    picked = [jnp.dot(p, returned, preferred_element_type=jnp.float32) for p in places]
    first_gate = (gw * jax.nn.sigmoid(gap))[:, None]
    second_gate = (gw * jax.nn.sigmoid(-gap))[:, None]
    result = (middle_wide + first_gate * picked[0] + second_gate * picked[1]).astype(jnp.bfloat16)
    return lax.all_to_all(result, "tp", split_axis=1, concat_axis=0, tiled=True)


def solution(mesh):
    return jax.shard_map(
        shards,
        mesh=mesh,
        in_specs=(
            P("sp", "tp"),
            P("sp", "tp"),
            P(None, "tp"),
            P("tp"),
            P("tp"),
            P("tp", None),
            P("sp", "tp"),
            P("tp"),
            P("sp", None),
            P("sp"),
            P("sp"),
            P("sp", None, "tp"),
            P("sp", None, "tp"),
            P("sp", "tp", None),
        ),
        out_specs=P("sp", "tp"),
        check_vma=False,
    )
```

```python
import functools

import jax
import jax.numpy as jnp
from jax import lax
from jax.experimental import pallas as pl
from jax.experimental.pallas import tpu as pltpu
from jax.sharding import PartitionSpec as P

MESH = pl.DeviceIdType.MESH
BF = jnp.bfloat16
F32 = jnp.float32
EPS = 1e-06
TAPS_PAD = 32
CHUNK = 64


def sigmoid(v):
    return jax.nn.sigmoid(v)


def kernel(
    S,
    T,
    cv,
    cg,
    cw,
    gain,
    shift,
    ow_hbm,
    res,
    mg,
    ids,
    gw,
    gap,
    wg_hbm,
    wu_hbm,
    wd_hbm,
    out,
    ow,
    wg,
    wu,
    wd,
    halo,
    gated,
    conv,
    st,
    stats,
    mv,
    part_s,
    part_r,
    res_r,
    mg_r,
    mid,
    place,
    og,
    rc,
    xb,
    hid,
    ys,
    yr,
    fin,
    loc,
    hsend,
    hrecv,
    tsend,
    trecv,
    wsend,
    wrecv,
    ssend,
    srecv,
    fsend,
    frecv,
):
    t = lax.axis_index("tp")
    s = lax.axis_index("sp")
    rows, chans = cv.shape
    taps = cw.shape[0]
    Q = rows // T
    feats = res.shape[1]
    D = feats * T
    cap = og.shape[1]
    hidden = wg.shape[2]
    slots = S * cap

    loads = [
        pltpu.make_async_copy(wg_hbm.at[0], wg.at[t], loc.at[0]),
        pltpu.make_async_copy(wu_hbm.at[0], wu.at[t], loc.at[1]),
        pltpu.make_async_copy(ow_hbm, ow, loc.at[2]),
    ]
    for c in range(T):
        loads.append(
            pltpu.make_async_copy(
                wd_hbm.at[0, :, pl.ds(c * feats, feats)], wd.at[c, t], loc.at[3 + c]
            )
        )
    for load in loads:
        load.start()

    barrier = pltpu.get_barrier_semaphore()

    @pl.loop(1, S)
    def _(k):
        pl.semaphore_signal(
            barrier, inc=1, device_id={"sp": lax.rem(s + k, S)}, device_id_type=MESH
        )

    for d in range(1, T):
        pl.semaphore_signal(
            barrier, inc=1, device_id={"tp": lax.rem(t + d, T)}, device_id_type=MESH
        )
    gated[TAPS_PAD:, :] = cv[...].astype(F32) * sigmoid(cg[...].astype(F32))
    pl.semaphore_wait(barrier, S - 1 + T - 1)

    def remote(src, dst, send, recv, axis, who):
        return pltpu.make_async_remote_copy(
            src_ref=src,
            dst_ref=dst,
            send_sem=send,
            recv_sem=recv,
            device_id={axis: who},
            device_id_type=MESH,
        )

    def tp_copy(kind, src, dst, d):
        return remote(src, dst, tsend.at[kind, d], trecv.at[kind, d], "tp", lax.rem(t + d, T))

    def half(unit, block, h):
        if unit == 0:
            n = wg.shape[1] // 2
            return wg.at[block, pl.ds(h * n, n), :]
        if unit == 1:
            n = wu.shape[1] // 2
            return wu.at[block, pl.ds(h * n, n), :]
        n = hidden // 2
        return wd.at[unit - 2, block, pl.ds(h * n, n), :]

    right, left = lax.rem(t + 1, T), lax.rem(t + T - 1, T)
    far = lax.rem(t + 2, T)

    def ring(unit, block, h, to_right, idx):
        ref = half(unit, block, h)
        return remote(
            ref, ref, wsend.at[unit, idx], wrecv.at[unit, idx], "tp", right if to_right else left
        )

    def direct(unit, h):
        for to_right in (True, False):
            ring(unit, t, h, to_right, 2 * h + (0 if to_right else 1)).start()

    def direct_wait(unit, h, from_left):
        ring(unit, left if from_left else right, h, True, 2 * h + (0 if from_left else 1)).wait_recv()

    def relay(unit):
        direct_wait(unit, 0, True)
        ring(unit, left, 0, True, 4).start()
        direct_wait(unit, 1, False)
        ring(unit, right, 1, False, 5).start()

    def near_wait(unit):
        direct_wait(unit, 1, True)
        direct_wait(unit, 0, False)

    def far_wait(unit):
        ring(unit, far, 0, True, 4).wait_recv()
        ring(unit, far, 1, True, 5).wait_recv()

    halo_copies = [
        remote(
            src.at[pl.ds(rows - TAPS_PAD, TAPS_PAD), :],
            halo.at[i],
            hsend.at[i],
            hrecv.at[i],
            "sp",
            lax.rem(s + 1, S),
        )
        for i, src in enumerate((cv, cg))
    ]
    for copy in halo_copies:
        copy.start()
    res_copies, gain_copies = [], []
    for d in range(1, T):
        peer = lax.rem(t + d, T)
        res_copies.append(tp_copy(0, res.at[pl.ds(peer * Q, Q), :], res_r.at[t], d))
        gain_copies.append(tp_copy(1, mg, mg_r.at[t], d))
    for copy in res_copies + gain_copies:
        copy.start()
    loads[0].wait()
    direct(0, 0)
    res_r[t] = res[pl.ds(t * Q, Q), :]
    mg_r[t] = mg[...]

    for copy in halo_copies:
        copy.wait_recv()
    first = jnp.where(s == 0, 0.0, 1.0).astype(F32)
    gated[:TAPS_PAD, :] = halo[0].astype(F32) * sigmoid(halo[1].astype(F32)) * first

    lane = lax.broadcasted_iota(jnp.int32, (CHUNK, 128), 1)

    @pl.loop(0, rows // CHUNK)
    def _(r):
        base = pl.multiple_of(r * CHUNK, CHUNK)
        span = CHUNK + TAPS_PAD
        window = gated[pl.ds(base, span), :]
        total = jnp.zeros((CHUNK, chans), F32)
        lead = TAPS_PAD - (taps - 1)
        for phase in range(8):
            turned = pltpu.roll(window, span - phase, 0) if phase else window
            for j in range(taps):
                if (lead + j) % 8 == phase:
                    at = lead + j - phase
                    total = total + cw[j : j + 1, :] * turned[at : at + CHUNK]
        conv[pl.ds(base, CHUNK), :] = total
        ssum = jnp.sum(total, axis=1, keepdims=True)
        ssq = jnp.sum(total * total, axis=1, keepdims=True)
        st[pl.ds(base, CHUNK), :] = jnp.where(lane == 0, ssum, jnp.where(lane == 1, ssq, 0.0))

    stats[t] = st[...].T[:8]
    stat_copies = [tp_copy(2, stats.at[t], stats.at[t], d) for d in range(1, T)]
    for copy in stat_copies:
        copy.start()
    direct(0, 1)

    here = pl.ds(pl.multiple_of(t * Q, Q), Q)
    E = S
    expert_iota = lax.broadcasted_iota(jnp.int32, (E, Q), 0)
    id_rows = [ids[k : k + 1, here] for k in range(2)]
    hits = [(expert_iota == id_rows[k]).astype(F32) for k in range(2)]
    upper = (
        lax.broadcasted_iota(jnp.int32, (Q, Q), 0) < lax.broadcasted_iota(jnp.int32, (Q, Q), 1)
    ).astype(BF)
    before = jnp.dot((hits[0] + hits[1]).astype(BF), upper, preferred_element_type=F32)
    slot_rows = [
        id_rows[k].astype(F32) * cap + jnp.sum(before * hits[k], axis=0, keepdims=True)
        for k in range(2)
    ]
    slot_iota = lax.broadcasted_iota(jnp.int32, (slots, Q), 0).astype(F32)
    send_matrix = jnp.where(
        (slot_iota == slot_rows[0]) | (slot_iota == slot_rows[1]), 1.0, 0.0
    ).astype(BF)
    weight = gw[:, here]
    gate_rows = [weight * sigmoid(gap[:, here]), weight * sigmoid(-gap[:, here])]
    table = jnp.concatenate(slot_rows + gate_rows + [jnp.zeros((Q - 4, Q), F32)], axis=0).T
    lane_iota = lax.broadcasted_iota(jnp.int32, (Q, slots), 1).astype(F32)
    for k in range(2):
        place[k] = jnp.where(lane_iota == table[:, k : k + 1], 1.0, 0.0).astype(BF)
    gates = [table[:, 2 + k : 3 + k] for k in range(2)]

    def tp_wait(kind, ref, d):
        remote(ref, ref, tsend.at[kind, d], trecv.at[kind, d], "tp", right).wait_recv()

    for d in range(1, T):
        tp_wait(2, stats.at[lax.rem(t + T - d, T)], d)
    whole = stats[0]
    for b in range(1, T):
        whole = whole + stats[b]
    whole = jnp.concatenate([whole, jnp.zeros((120, rows), F32)], axis=0).T
    mean = whole[:, 0:1] / (chans * T)
    var = whole[:, 1:2] / (chans * T) - mean * mean
    wide = lax.broadcasted_iota(jnp.int32, (rows, 128), 1)
    mv[...] = jnp.where(wide == 0, mean, lax.rsqrt(var + EPS))

    loads[2].wait()

    def project(q, dst):
        at = pl.ds(pl.multiple_of(q * Q, Q), Q)
        stat = mv[at, :]
        normal = (conv[at, :] - stat[:, 0:1]) * stat[:, 1:2] * gain[...] + shift[...]
        act = (normal * sigmoid(normal)).astype(BF)
        for c in range(T):
            cols = pl.ds(c * feats, feats)
            dst[:, cols] = jnp.dot(act, ow[:, cols], preferred_element_type=F32).astype(BF)

    part_copies = []
    for d in (2, 1, 3):
        peer = lax.rem(t + d, T)
        project(peer, part_s.at[d])
        copy = tp_copy(3, part_s.at[d], part_r.at[t], d)
        copy.start()
        part_copies.append(copy)
    project(t, part_r.at[t])

    relay(0)
    loads[1].wait()
    direct(1, 0)
    direct(1, 1)

    for d in range(1, T):
        b = lax.rem(t + T - d, T)
        tp_wait(0, res_r.at[b], d)
        tp_wait(1, mg_r.at[b], d)
        tp_wait(3, part_r.at[b], d)
    square = jnp.zeros((Q, 1), F32)
    for c in range(T):
        cols = pl.ds(c * feats, feats)
        mixed = part_r[0, :, cols].astype(F32)
        for b in range(1, T):
            mixed = mixed + part_r[b, :, cols].astype(F32)
        middle = (res_r[c].astype(F32) + mixed).astype(BF)
        mid[:, cols] = middle
        middle = middle.astype(F32)
        square = square + jnp.sum(middle * middle, axis=1, keepdims=True)
    scale = lax.rsqrt(square / D + EPS)
    for c in range(T):
        cols = pl.ds(c * feats, feats)
        normed = (mid[:, cols].astype(F32) * scale * mg_r[c]).astype(BF)
        sent = jnp.dot(send_matrix, normed, preferred_element_type=F32)
        og[:, :, cols] = sent.reshape(S, cap, feats).astype(BF)
    rc[s] = og[s]

    def sp_exchange(src, dst, send, recv):
        def one(k):
            peer = lax.rem(s + k, S)
            remote(src.at[peer], dst.at[s], send, recv, "sp", peer).start()

        one(S // 2)

        @pl.loop(1, S // 2)
        def _(i):
            one(S // 2 - i)
            one(S // 2 + i)

    def sp_wait(ref, send, recv):
        many = ref.at[pl.ds(0, S - 1)]
        return remote(many, many, send, recv, "tp", right)

    sp_exchange(og, rc, ssend.at[T], srecv.at[T])

    relay(1)
    for c in range(T):
        loads[3 + c].wait()
        direct(2 + c, 0)
        direct(2 + c, 1)
    near_wait(0)
    far_wait(0)
    near_wait(1)
    sp_wait(rc, ssend.at[T], srecv.at[T]).wait_recv()
    for c in range(T):
        cols = pl.ds(c * feats, feats)
        xb[:, cols] = rc[:, :, cols].astype(F32).reshape(slots, feats).astype(BF)

    def expert(b):
        g = jnp.dot(xb[...], wg[b], preferred_element_type=F32)
        u = jnp.dot(xb[...], wu[b], preferred_element_type=F32)
        hid[b] = (g * sigmoid(g) * u).astype(BF)

    relay(2)

    @pl.loop(0, T - 1)
    def _(i):
        expert(lax.rem(t + T - 1 + i, T))

    far_wait(1)
    for c in range(1, T):
        relay(2 + c)
    expert(far)

    for c in range(T):
        near_wait(2 + c)
        far_wait(2 + c)

        @pl.loop(0, 2)
        def _(r, c=c):
            n = slots // 2
            at = pl.ds(pl.multiple_of(r * n, n), n)
            total = jnp.zeros((n, feats), F32)
            for b in range(T):
                term = jnp.dot(hid[b, at, :], wd[c, b], preferred_element_type=F32)
                total = total + term.astype(BF).astype(F32)
            ys[c, pl.ds(r * (S // 2), S // 2)] = total.reshape(S // 2, cap, feats).astype(BF)

        yr[c, s] = ys[c, s]
        sp_exchange(ys.at[c], yr.at[c], ssend.at[c], srecv.at[c])

    for c in range(T):
        sp_wait(yr.at[c], ssend.at[c], srecv.at[c]).wait_recv()
        back = yr[c].astype(F32).reshape(slots, feats).astype(BF)
        cols = pl.ds(c * feats, feats)
        result = mid[:, cols].astype(F32)
        for k in range(2):
            result = result + gates[k] * jnp.dot(place[k], back, preferred_element_type=F32)
        fin[c] = result.astype(BF)
        mine = pl.ds(pl.multiple_of(t * Q, Q), Q)

        @pl.when(t != c)
        def _(c=c):
            remote(fin.at[c], out.at[mine, :], fsend.at[c], frecv.at[t], "tp", c).start()

        @pl.when(t == c)
        def _(c=c):
            out[mine, :] = fin[c]

    for c in range(T):

        @pl.when(t != c)
        def _(c=c):
            remote(fin.at[c], fin.at[c], fsend.at[c], frecv.at[c], "tp", c).wait_send()
            theirs = out.at[pl.ds(c * Q, Q), :]
            remote(theirs, theirs, fsend.at[c], frecv.at[c], "tp", c).wait_recv()

        sp_wait(ys.at[c], ssend.at[c], srecv.at[c]).wait_send()
    sp_wait(og, ssend.at[T], srecv.at[T]).wait_send()
    for copy in halo_copies + res_copies + gain_copies + stat_copies + part_copies:
        copy.wait_send()
    for unit in range(2 + T):
        for h in range(2):
            for i in range(2):
                ring(unit, t, h, True, 2 * h + i).wait_send()
        ring(unit, left, 0, True, 4).wait_send()
        ring(unit, right, 1, True, 5).wait_send()


def shards(
    conv_value,
    conv_gate,
    conv_weight,
    conv_gain,
    conv_shift,
    out_weight,
    residual,
    mix_gain,
    expert_ids,
    group_weight,
    score_gap,
    w_gate,
    w_up,
    w_down,
):
    S, T = lax.axis_size("sp"), lax.axis_size("tp")
    rows, chans = conv_value.shape
    feats = residual.shape[1]
    D = feats * T
    Q = rows // T
    cap = 4 * Q // S
    slots = S * cap
    hidden = w_gate.shape[2]
    vm = pl.BlockSpec(memory_space=pltpu.VMEM)
    hbm = pl.BlockSpec(memory_space=pl.ANY)
    dma = pltpu.SemaphoreType.DMA
    return pl.pallas_call(
        functools.partial(kernel, S, T),
        name="layer",
        out_shape=jax.ShapeDtypeStruct((rows, feats), BF),
        in_specs=[vm] * 5 + [hbm] + [vm] * 5 + [hbm] * 3,
        out_specs=vm,
        scratch_shapes=[
            pltpu.VMEM(out_weight.shape, BF),
            pltpu.VMEM((T, D, hidden), BF),
            pltpu.VMEM((T, D, hidden), BF),
            pltpu.VMEM((T, T, hidden, feats), BF),
            pltpu.VMEM((2, TAPS_PAD, chans), BF),
            pltpu.VMEM((rows + TAPS_PAD, chans), F32),
            pltpu.VMEM((rows, chans), F32),
            pltpu.VMEM((rows, 128), F32),
            pltpu.VMEM((T, 8, rows), F32),
            pltpu.VMEM((rows, 128), F32),
            pltpu.VMEM((T, Q, D), BF),
            pltpu.VMEM((T, Q, D), BF),
            pltpu.VMEM((T, Q, feats), BF),
            pltpu.VMEM((T, 1, feats), F32),
            pltpu.VMEM((Q, D), BF),
            pltpu.VMEM((2, Q, slots), BF),
            pltpu.VMEM((S, cap, D), BF),
            pltpu.VMEM((S, cap, D), BF),
            pltpu.VMEM((slots, D), BF),
            pltpu.VMEM((T, slots, hidden), BF),
            pltpu.VMEM((T, S, cap, feats), BF),
            pltpu.VMEM((T, S, cap, feats), BF),
            pltpu.VMEM((T, Q, feats), BF),
            dma((3 + T,)),
            dma((2,)),
            dma((2,)),
            dma((4, T)),
            dma((4, T)),
            dma((2 + T, 6)),
            dma((2 + T, 6)),
            dma((T + 1,)),
            dma((T + 1,)),
            dma((T,)),
            dma((T,)),
        ],
        compiler_params=pltpu.CompilerParams(
            collective_id=0, has_side_effects=True, vmem_limit_bytes=60 * 1024 * 1024
        ),
    )(
        conv_value,
        conv_gate,
        conv_weight,
        conv_gain.reshape(1, -1),
        conv_shift.reshape(1, -1),
        out_weight,
        residual,
        mix_gain.reshape(1, -1),
        expert_ids.T,
        group_weight.reshape(1, -1),
        score_gap.reshape(1, -1),
        w_gate,
        w_up,
        w_down,
    )


def solution(mesh):
    return jax.shard_map(
        shards,
        mesh=mesh,
        in_specs=(
            P("sp", "tp"),
            P("sp", "tp"),
            P(None, "tp"),
            P("tp"),
            P("tp"),
            P("tp", None),
            P("sp", "tp"),
            P("tp"),
            P("sp", None),
            P("sp"),
            P("sp"),
            P("sp", None, "tp"),
            P("sp", None, "tp"),
            P("sp", "tp", None),
        ),
        out_specs=P("sp", "tp"),
        check_vma=False,
    )
```

```python
import functools

import jax
import jax.numpy as jnp
from jax import lax
from jax.experimental import pallas as pl
from jax.experimental.pallas import tpu as pltpu
from jax.sharding import PartitionSpec as P

MESH = pl.DeviceIdType.MESH
BF = jnp.bfloat16
F32 = jnp.float32
EPS = 1e-06
TAPS_PAD = 32
CHUNK = 64
XS = 4
CORES = 2


def sigmoid(v):
    return jax.nn.sigmoid(v)


def kernel(
    S,
    T,
    cv,
    cg,
    cw,
    gain,
    shift,
    ow_hbm,
    res,
    mg,
    ids,
    gw,
    gap,
    wg_hbm,
    wu_hbm,
    wd_hbm,
    out,
    ow,
    wg,
    wu,
    wd,
    halo,
    gated,
    conv,
    st,
    stats,
    mv,
    act_s,
    act_r,
    res_r,
    mg_r,
    mid,
    place,
    og,
    rc,
    xb,
    hid,
    ys,
    yr,
    fin,
    loc,
    hsend,
    hrecv,
    tsend,
    trecv,
    osend,
    orecv,
    wsend,
    wrecv,
    ssend,
    srecv,
    fsend,
    frecv,
):
    t = lax.axis_index("tp")
    s = lax.axis_index("sp")
    rows, chans = cv.shape
    taps = cw.shape[0]
    Q = rows // T
    feats = res.shape[1]
    D = feats * T
    cap = og.shape[1]
    hidden = wg.shape[2]
    slots = S * cap
    strip = feats // T
    core = lax.rem(s, CORES)
    x = lax.rem(s // CORES, XS)
    line = s - core - x * CORES
    x_right, x_left = lax.rem(x + 1, XS), lax.rem(x + XS - 1, XS)
    x_far = lax.rem(x + 2, XS)

    loads = [pltpu.make_async_copy(ow_hbm, ow.at[t], loc.at[0])]
    loads.append(pltpu.make_async_copy(wg_hbm.at[0], wg.at[t], loc.at[1]))
    loads.append(pltpu.make_async_copy(wu_hbm.at[0], wu.at[t], loc.at[2]))
    for c in range(T):
        for j in range(T):
            loads.append(
                pltpu.make_async_copy(
                    wd_hbm.at[0, :, pl.ds(j * feats + c * strip, strip)],
                    wd.at[c, t, :, pl.ds(j * strip, strip)],
                    loc.at[3 + c * T + j],
                )
            )
    for load in loads:
        load.start()

    barrier = pltpu.get_barrier_semaphore()

    @pl.loop(1, S)
    def _(k):
        pl.semaphore_signal(
            barrier, inc=1, device_id={"sp": lax.rem(s + k, S)}, device_id_type=MESH
        )

    for d in range(1, T):
        pl.semaphore_signal(
            barrier, inc=1, device_id={"tp": lax.rem(t + d, T)}, device_id_type=MESH
        )
    gated[TAPS_PAD:, :] = cv[...].astype(F32) * sigmoid(cg[...].astype(F32))
    pl.semaphore_wait(barrier, S - 1 + T - 1)

    def remote(src, dst, send, recv, axis, who):
        return pltpu.make_async_remote_copy(
            src_ref=src,
            dst_ref=dst,
            send_sem=send,
            recv_sem=recv,
            device_id={axis: who},
            device_id_type=MESH,
        )

    right, left = lax.rem(t + 1, T), lax.rem(t + T - 1, T)
    far = lax.rem(t + 2, T)

    def tp_copy(kind, src, dst, d):
        return remote(src, dst, tsend.at[kind, d], trecv.at[kind, d], "tp", lax.rem(t + d, T))

    def tp_wait(kind, ref, d):
        remote(ref, ref, tsend.at[kind, d], trecv.at[kind, d], "tp", right).wait_recv()

    def half(unit, block, h):
        if unit < 4:
            ref = wg if unit < 2 else wu
            n = ref.shape[1] // 4
            return ref.at[block, pl.ds((unit % 2) * 2 * n + h * n, n), :]
        n = hidden // 2
        return wd.at[unit - 4, block, pl.ds(h * n, n), :]

    def ring(unit, block, h, to_right, idx):
        ref = half(unit, block, h)
        return remote(
            ref, ref, wsend.at[unit, idx], wrecv.at[unit, idx], "tp", right if to_right else left
        )

    def direct(unit):
        if unit >= 4:
            for j in range(T):
                loads[3 + (unit - 4) * T + j].wait()
        for h in range(2):
            ring(unit, t, h, True, 2 * h).start()
            ring(unit, t, 1 - h, False, 2 * (1 - h) + 1).start()

    def direct_wait(unit, h, from_left):
        ring(unit, left if from_left else right, h, True, 2 * h + (0 if from_left else 1)).wait_recv()

    def relay(unit):
        direct_wait(unit, 0, True)
        ring(unit, left, 0, True, 4).start()
        direct_wait(unit, 1, False)
        ring(unit, right, 1, False, 5).start()

    def near_wait(unit):
        direct_wait(unit, 1, True)
        direct_wait(unit, 0, False)

    def far_wait(unit):
        ring(unit, far, 0, True, 4).wait_recv()
        ring(unit, far, 1, True, 5).wait_recv()

    per = ow.shape[1] // (XS * CORES)

    def piece(block, at_x, at_core, h=None):
        base = (at_x * CORES + at_core) * per
        if h is None:
            return ow.at[block, pl.ds(base, per), :]
        return ow.at[block, pl.ds(base + h * (per // 2), per // 2), :]

    def from_block(d):
        return lax.rem(t + T - d, T)

    def share(kind, d, ref, who):
        return remote(ref, ref, osend.at[kind, d], orecv.at[kind, d], "sp", who)

    to_x_right = line + x_right * CORES + core
    to_x_left = line + x_left * CORES + core
    other = line + x * CORES + 1 - core
    sends = []

    def go(copy):
        copy.start()
        sends.append(copy)

    for i, src in enumerate((cv, cg)):
        go(
            remote(
                src.at[pl.ds(rows - TAPS_PAD, TAPS_PAD), :],
                halo.at[i],
                hsend.at[i],
                hrecv.at[i],
                "sp",
                lax.rem(s + 1, S),
            )
        )
    loads[0].wait()
    for d in range(1, T):
        mine = piece(t, x, core)
        go(tp_copy(3, mine, mine, d))
    for d in range(1, T):
        go(tp_copy(0, res.at[pl.ds(lax.rem(t + d, T) * Q, Q), :], res_r.at[t], d))
        go(tp_copy(1, mg, mg_r.at[t], d))
    res_r[t] = res[pl.ds(t * Q, Q), :]
    mg_r[t] = mg[...]

    for i in range(2):
        remote(halo.at[i], halo.at[i], hsend.at[i], hrecv.at[i], "tp", right).wait_recv()
    first = jnp.where(s == 0, 0.0, 1.0).astype(F32)
    gated[:TAPS_PAD, :] = halo[0].astype(F32) * sigmoid(halo[1].astype(F32)) * first

    lane = lax.broadcasted_iota(jnp.int32, (CHUNK, 128), 1)

    @pl.loop(0, rows // CHUNK)
    def _(r):
        base = pl.multiple_of(r * CHUNK, CHUNK)
        span = CHUNK + TAPS_PAD
        window = gated[pl.ds(base, span), :]
        total = jnp.zeros((CHUNK, chans), F32)
        lead = TAPS_PAD - (taps - 1)
        for phase in range(8):
            turned = pltpu.roll(window, span - phase, 0) if phase else window
            for j in range(taps):
                if (lead + j) % 8 == phase:
                    at = lead + j - phase
                    total = total + cw[j : j + 1, :] * turned[at : at + CHUNK]
        conv[pl.ds(base, CHUNK), :] = total
        ssum = jnp.sum(total, axis=1, keepdims=True)
        ssq = jnp.sum(total * total, axis=1, keepdims=True)
        st[pl.ds(base, CHUNK), :] = jnp.where(lane == 0, ssum, jnp.where(lane == 1, ssq, 0.0))

    stats[t] = st[...].T[:8]
    for d in range(1, T):
        go(tp_copy(2, stats.at[t], stats.at[t], d))

    for d in range(1, T):
        b = from_block(d)
        tp_wait(3, piece(b, x, core), d)
        go(share(0, d, piece(b, x, core), to_x_right))
        go(share(1, d, piece(b, x, core), to_x_left))
        go(share(4, d, piece(b, x, core), other))
    loads[1].wait()
    direct(0)

    here = pl.ds(pl.multiple_of(t * Q, Q), Q)
    E = S
    expert_iota = lax.broadcasted_iota(jnp.int32, (E, Q), 0)
    id_rows = [ids[k : k + 1, here] for k in range(2)]
    hits = [(expert_iota == id_rows[k]).astype(F32) for k in range(2)]
    upper = (
        lax.broadcasted_iota(jnp.int32, (Q, Q), 0) < lax.broadcasted_iota(jnp.int32, (Q, Q), 1)
    ).astype(BF)
    before = jnp.dot((hits[0] + hits[1]).astype(BF), upper, preferred_element_type=F32)
    slot_rows = [
        id_rows[k].astype(F32) * cap + jnp.sum(before * hits[k], axis=0, keepdims=True)
        for k in range(2)
    ]
    slot_iota = lax.broadcasted_iota(jnp.int32, (slots, Q), 0).astype(F32)
    send_matrix = jnp.where(
        (slot_iota == slot_rows[0]) | (slot_iota == slot_rows[1]), 1.0, 0.0
    ).astype(BF)
    weight = gw[:, here]
    gate_rows = [weight * sigmoid(gap[:, here]), weight * sigmoid(-gap[:, here])]
    table = jnp.concatenate(slot_rows + gate_rows + [jnp.zeros((Q - 4, Q), F32)], axis=0).T
    lane_iota = lax.broadcasted_iota(jnp.int32, (Q, slots), 1).astype(F32)
    for k in range(2):
        place[k] = jnp.where(lane_iota == table[:, k : k + 1], 1.0, 0.0).astype(BF)
    gates = [table[:, 2 + k : 3 + k] for k in range(2)]

    for d in range(1, T):
        tp_wait(2, stats.at[from_block(d)], d)
    whole = stats[0]
    for b in range(1, T):
        whole = whole + stats[b]
    whole = jnp.concatenate([whole, jnp.zeros((120, rows), F32)], axis=0).T
    mean = whole[:, 0:1] / (chans * T)
    var = whole[:, 1:2] / (chans * T) - mean * mean
    wide = lax.broadcasted_iota(jnp.int32, (rows, 128), 1)
    mv[...] = jnp.where(wide == 0, mean, lax.rsqrt(var + EPS))

    def activate(q, dst):
        at = pl.ds(pl.multiple_of(q * Q, Q), Q)
        stat = mv[at, :]
        normal = (conv[at, :] - stat[:, 0:1]) * stat[:, 1:2] * gain[...] + shift[...]
        dst[...] = (normal * sigmoid(normal)).astype(BF)

    for d in (2, 1, 3):
        activate(lax.rem(t + d, T), act_s.at[d])
        go(tp_copy(4, act_s.at[d], act_r.at[t], d))
    activate(t, act_r.at[t])
    direct(1)

    for d in range(1, T):
        b = from_block(d)
        near = piece(b, x_left, core)
        share(0, d, near, other).wait_recv()
        go(share(2, d, piece(b, x_left, core, 0), to_x_right))
        go(share(5, d, near, other))
    for d in range(1, T):
        b = from_block(d)
        near = piece(b, x_right, core)
        share(1, d, near, other).wait_recv()
        go(share(3, d, piece(b, x_right, core, 1), to_x_left))
        go(share(6, d, near, other))
    for d in range(1, T):
        b = from_block(d)
        share(2, d, piece(b, x_far, core, 0), other).wait_recv()
        share(3, d, piece(b, x_far, core, 1), other).wait_recv()
        go(share(7, d, piece(b, x_far, core), other))

    for d in range(1, T):
        b = from_block(d)
        tp_wait(0, res_r.at[b], d)
        tp_wait(1, mg_r.at[b], d)
        tp_wait(4, act_r.at[b], d)
    for i, at_x in enumerate((x, x_left, x_right, x_far)):
        for d in range(1, T):
            share(4 + i, d, piece(from_block(d), at_x, 1 - core), other).wait_recv()

    square = jnp.zeros((Q, 1), F32)
    for c in range(T):
        cols = pl.ds(c * feats, feats)
        mixed = jnp.zeros((Q, feats), F32)
        for b in range(T):
            term = jnp.dot(act_r[b], ow[b, :, cols], preferred_element_type=F32)
            mixed = mixed + term.astype(BF).astype(F32)
        middle = (res_r[c].astype(F32) + mixed).astype(BF)
        mid[:, cols] = middle
        middle = middle.astype(F32)
        square = square + jnp.sum(middle * middle, axis=1, keepdims=True)
    scale = lax.rsqrt(square / D + EPS)
    for c in range(T):
        cols = pl.ds(c * feats, feats)
        normed = (mid[:, cols].astype(F32) * scale * mg_r[c]).astype(BF)
        sent = jnp.dot(send_matrix, normed, preferred_element_type=F32)
        og[:, :, cols] = sent.reshape(S, cap, feats).astype(BF)
    rc[s] = og[s]

    def sp_exchange(src, dst, send, recv):
        def one(k):
            peer = lax.rem(s + k, S)
            remote(src.at[peer], dst.at[s], send, recv, "sp", peer).start()

        one(S // 2)

        @pl.loop(1, S // 2)
        def _(i):
            one(S // 2 - i)
            one(S // 2 + i)

    def sp_wait(ref, send, recv):
        many = ref.at[pl.ds(0, S - 1)]
        return remote(many, many, send, recv, "tp", right)

    sp_exchange(og, rc, ssend.at[T], srecv.at[T])

    relay(0)
    loads[2].wait()
    direct(2)
    relay(1)
    direct(3)
    relay(2)
    direct(4)
    relay(3)
    relay(4)
    direct(5)
    direct(6)
    for unit in range(4):
        near_wait(unit)
    far_wait(0)
    far_wait(1)
    sp_wait(rc, ssend.at[T], srecv.at[T]).wait_recv()
    for c in range(T):
        cols = pl.ds(c * feats, feats)
        xb[:, cols] = rc[:, :, cols].astype(F32).reshape(slots, feats).astype(BF)

    def expert(b):
        g = jnp.dot(xb[...], wg[b], preferred_element_type=F32)
        u = jnp.dot(xb[...], wu[b], preferred_element_type=F32)
        hid[b] = (g * sigmoid(g) * u).astype(BF)

    @pl.loop(0, T - 1)
    def _(i):
        expert(lax.rem(t + T - 1 + i, T))

    far_wait(2)
    far_wait(3)
    expert(far)

    for c in range(T):
        if c + 1 < T:
            relay(5 + c)
        if c == 0:
            direct(7)
        near_wait(4 + c)
        far_wait(4 + c)

        @pl.loop(0, 2)
        def _(r, c=c):
            n = slots // 2
            at = pl.ds(pl.multiple_of(r * n, n), n)
            total = jnp.zeros((n, feats), F32)
            for b in range(T):
                term = jnp.dot(hid[b, at, :], wd[c, b], preferred_element_type=F32)
                total = total + term.astype(BF).astype(F32)
            ys[c, pl.ds(r * (S // 2), S // 2)] = total.reshape(S // 2, cap, feats).astype(BF)

        yr[c, s] = ys[c, s]
        sp_exchange(ys.at[c], yr.at[c], ssend.at[c], srecv.at[c])

    my_rows = pl.ds(pl.multiple_of(t * Q, Q), Q)
    for c in range(T):
        sp_wait(yr.at[c], ssend.at[c], srecv.at[c]).wait_recv()
        back = yr[c].astype(F32).reshape(slots, feats).astype(BF)
        picked = [jnp.dot(place[k], back, preferred_element_type=F32) for k in range(2)]
        added = gates[0] * picked[0] + gates[1] * picked[1]
        for j in range(T):
            middle = mid[:, pl.ds(j * feats + c * strip, strip)].astype(F32)
            fin[c, j] = (middle + added[:, j * strip : (j + 1) * strip]).astype(BF)
        cols = pl.ds(c * strip, strip)
        for d in range(1, T):
            peer = lax.rem(t + d, T)
            go(remote(fin.at[c, peer], out.at[my_rows, cols], fsend.at[c, d], frecv.at[c, d], "tp", peer))
        out[my_rows, cols] = fin[c, t]

    for c in range(T):
        sp_wait(ys.at[c], ssend.at[c], srecv.at[c]).wait_send()
    sp_wait(og, ssend.at[T], srecv.at[T]).wait_send()
    for copy in sends:
        copy.wait_send()
    for unit in range(4 + T):
        for idx in range(4):
            ring(unit, t, idx // 2, True, idx).wait_send()
        ring(unit, left, 0, True, 4).wait_send()
        ring(unit, right, 1, True, 5).wait_send()
    for c in range(T):
        for d in range(1, T):
            theirs = out.at[pl.ds(from_block(d) * Q, Q), pl.ds(c * strip, strip)]
            remote(theirs, theirs, fsend.at[c, d], frecv.at[c, d], "tp", right).wait_recv()


def shards(
    conv_value,
    conv_gate,
    conv_weight,
    conv_gain,
    conv_shift,
    out_weight,
    residual,
    mix_gain,
    expert_ids,
    group_weight,
    score_gap,
    w_gate,
    w_up,
    w_down,
):
    S, T = lax.axis_size("sp"), lax.axis_size("tp")
    rows, chans = conv_value.shape
    feats = residual.shape[1]
    D = feats * T
    Q = rows // T
    cap = 4 * Q // S
    slots = S * cap
    hidden = w_gate.shape[2]
    vm = pl.BlockSpec(memory_space=pltpu.VMEM)
    hbm = pl.BlockSpec(memory_space=pl.ANY)
    dma = pltpu.SemaphoreType.DMA
    return pl.pallas_call(
        functools.partial(kernel, S, T),
        name="layer",
        out_shape=jax.ShapeDtypeStruct((rows, feats), BF),
        in_specs=[vm] * 5 + [hbm] + [vm] * 5 + [hbm] * 3,
        out_specs=vm,
        scratch_shapes=[
            pltpu.VMEM((T, chans, D), BF),
            pltpu.VMEM((T, D, hidden), BF),
            pltpu.VMEM((T, D, hidden), BF),
            pltpu.VMEM((T, T, hidden, feats), BF),
            pltpu.VMEM((2, TAPS_PAD, chans), BF),
            pltpu.VMEM((rows + TAPS_PAD, chans), F32),
            pltpu.VMEM((rows, chans), F32),
            pltpu.VMEM((rows, 128), F32),
            pltpu.VMEM((T, 8, rows), F32),
            pltpu.VMEM((rows, 128), F32),
            pltpu.VMEM((T, Q, chans), BF),
            pltpu.VMEM((T, Q, chans), BF),
            pltpu.VMEM((T, Q, feats), BF),
            pltpu.VMEM((T, 1, feats), F32),
            pltpu.VMEM((Q, D), BF),
            pltpu.VMEM((2, Q, slots), BF),
            pltpu.VMEM((S, cap, D), BF),
            pltpu.VMEM((S, cap, D), BF),
            pltpu.VMEM((slots, D), BF),
            pltpu.VMEM((T, slots, hidden), BF),
            pltpu.VMEM((T, S, cap, feats), BF),
            pltpu.VMEM((T, S, cap, feats), BF),
            pltpu.VMEM((T, T, Q, feats // T), BF),
            dma((3 + T * T,)),
            dma((2,)),
            dma((2,)),
            dma((5, T)),
            dma((5, T)),
            dma((8, T)),
            dma((8, T)),
            dma((4 + T, 6)),
            dma((4 + T, 6)),
            dma((T + 1,)),
            dma((T + 1,)),
            dma((T, T)),
            dma((T, T)),
        ],
        compiler_params=pltpu.CompilerParams(
            collective_id=0, has_side_effects=True, vmem_limit_bytes=60 * 1024 * 1024
        ),
    )(
        conv_value,
        conv_gate,
        conv_weight,
        conv_gain.reshape(1, -1),
        conv_shift.reshape(1, -1),
        out_weight,
        residual,
        mix_gain.reshape(1, -1),
        expert_ids.T,
        group_weight.reshape(1, -1),
        score_gap.reshape(1, -1),
        w_gate,
        w_up,
        w_down,
    )


def solution(mesh):
    return jax.shard_map(
        shards,
        mesh=mesh,
        in_specs=(
            P("sp", "tp"),
            P("sp", "tp"),
            P(None, "tp"),
            P("tp"),
            P("tp"),
            P("tp", None),
            P("sp", "tp"),
            P("tp"),
            P("sp", None),
            P("sp"),
            P("sp"),
            P("sp", None, "tp"),
            P("sp", None, "tp"),
            P("sp", "tp", None),
        ),
        out_specs=P("sp", "tp"),
        check_vma=False,
    )
```

```python
import functools

import jax
import jax.numpy as jnp
from jax import lax
from jax.experimental import pallas as pl
from jax.experimental.pallas import tpu as pltpu
from jax.sharding import PartitionSpec as P

MESH = pl.DeviceIdType.MESH
BF = jnp.bfloat16
F32 = jnp.float32
EPS = 1e-06
TAPS_PAD = 32
CHUNK = 64
CHUNKS = 8
XS = 4
CORES = 2


def sigmoid(v):
    return jax.nn.sigmoid(v)


def kernel(
    S,
    T,
    cv,
    cg,
    cw,
    gain,
    shift,
    ow_hbm,
    res,
    mg,
    ids,
    gw,
    gap,
    wg_hbm,
    wu_hbm,
    wd_hbm,
    out,
    ow,
    wg,
    wu,
    wd,
    halo,
    gated,
    conv,
    st,
    stats,
    mv,
    act_s,
    act_r,
    res_r,
    mg_r,
    mid,
    place,
    og,
    rc,
    xb,
    hid,
    ys,
    yr,
    fin,
    loc,
    hsend,
    hrecv,
    tsend,
    trecv,
    osend,
    orecv,
    wsend,
    wrecv,
    ssend,
    srecv,
    fsend,
    frecv,
):
    t = lax.axis_index("tp")
    s = lax.axis_index("sp")
    rows, chans = cv.shape
    taps = cw.shape[0]
    Q = rows // T
    feats = res.shape[1]
    D = feats * T
    cap = og.shape[1]
    hidden = wg.shape[2]
    chunks = ys.shape[0]
    width = D // chunks
    per_chunk = width // 128
    blocks_by = T // per_chunk
    slots = S * cap
    strip = 128
    core = lax.rem(s, CORES)
    x = lax.rem(s // CORES, XS)
    base = s - core - x * CORES
    depth = S // (XS * CORES)
    z = base // (XS * CORES)
    xp, zp = lax.rem(x, 2), lax.rem(z, 2)
    x_right = base + lax.rem(x + 1, XS) * CORES + core
    x_left = base + lax.rem(x + XS - 1, XS) * CORES + core
    z_right = lax.rem(z + 1, depth) * (XS * CORES) + x * CORES + core
    z_left = lax.rem(z + depth - 1, depth) * (XS * CORES) + x * CORES + core
    other = s + 1 - 2 * core

    loads = [pltpu.make_async_copy(ow_hbm, ow.at[t], loc.at[0])]
    loads.append(pltpu.make_async_copy(wg_hbm.at[0], wg.at[t], loc.at[1]))
    loads.append(pltpu.make_async_copy(wu_hbm.at[0], wu.at[t], loc.at[2]))

    def columns(c, i):
        block = (c % blocks_by) * per_chunk + i
        return block, block * feats + (c // blocks_by) * strip

    for c in range(chunks):
        for i in range(per_chunk):
            loads.append(
                pltpu.make_async_copy(
                    wd_hbm.at[0, :, pl.ds(columns(c, i)[1], strip)],
                    wd.at[c, t, :, pl.ds(i * strip, strip)],
                    loc.at[3 + c * per_chunk + i],
                )
            )
    for load in loads:
        load.start()

    barrier = pltpu.get_barrier_semaphore()

    @pl.loop(1, S)
    def _(k):
        pl.semaphore_signal(
            barrier, inc=1, device_id={"sp": lax.rem(s + k, S)}, device_id_type=MESH
        )

    for d in range(1, T):
        pl.semaphore_signal(
            barrier, inc=1, device_id={"tp": lax.rem(t + d, T)}, device_id_type=MESH
        )
    gated[TAPS_PAD:, :] = cv[...].astype(F32) * sigmoid(cg[...].astype(F32))
    lane = lax.broadcasted_iota(jnp.int32, (CHUNK, 128), 1)

    def conv_rows(r):
        base = r * CHUNK if isinstance(r, int) else pl.multiple_of(r * CHUNK, CHUNK)
        span = CHUNK + TAPS_PAD
        window = gated[pl.ds(base, span), :]
        total = jnp.zeros((CHUNK, chans), F32)
        lead = TAPS_PAD - (taps - 1)
        for phase in range(8):
            turned = pltpu.roll(window, span - phase, 0) if phase else window
            for j in range(taps):
                if (lead + j) % 8 == phase:
                    at = lead + j - phase
                    total = total + cw[j : j + 1, :] * turned[at : at + CHUNK]
        conv[pl.ds(base, CHUNK), :] = total
        ssum = jnp.sum(total, axis=1, keepdims=True)
        ssq = jnp.sum(total * total, axis=1, keepdims=True)
        st[pl.ds(base, CHUNK), :] = jnp.where(lane == 0, ssum, jnp.where(lane == 1, ssq, 0.0))

    @pl.loop(1, rows // CHUNK)
    def _(r):
        conv_rows(r)

    here = pl.ds(pl.multiple_of(t * Q, Q), Q)
    E = S
    expert_iota = lax.broadcasted_iota(jnp.int32, (E, Q), 0)
    id_rows = [ids[k : k + 1, here] for k in range(2)]
    hits = [(expert_iota == id_rows[k]).astype(F32) for k in range(2)]
    upper = (
        lax.broadcasted_iota(jnp.int32, (Q, Q), 0) < lax.broadcasted_iota(jnp.int32, (Q, Q), 1)
    ).astype(BF)
    before = jnp.dot((hits[0] + hits[1]).astype(BF), upper, preferred_element_type=F32)
    slot_rows = [
        id_rows[k].astype(F32) * cap + jnp.sum(before * hits[k], axis=0, keepdims=True)
        for k in range(2)
    ]
    slot_iota = lax.broadcasted_iota(jnp.int32, (slots, Q), 0).astype(F32)
    send_matrix = jnp.where(
        (slot_iota == slot_rows[0]) | (slot_iota == slot_rows[1]), 1.0, 0.0
    ).astype(BF)
    weight = gw[:, here]
    gate_rows = [weight * sigmoid(gap[:, here]), weight * sigmoid(-gap[:, here])]
    table = jnp.concatenate(slot_rows + gate_rows + [jnp.zeros((Q - 4, Q), F32)], axis=0).T
    lane_iota = lax.broadcasted_iota(jnp.int32, (Q, slots), 1).astype(F32)
    for k in range(2):
        place[k] = jnp.where(lane_iota == table[:, k : k + 1], 1.0, 0.0).astype(BF)
    gates = [table[:, 2 + k : 3 + k] for k in range(2)]

    pl.semaphore_wait(barrier, S - 1 + T - 1)

    def remote(src, dst, send, recv, axis, who):
        return pltpu.make_async_remote_copy(
            src_ref=src,
            dst_ref=dst,
            send_sem=send,
            recv_sem=recv,
            device_id={axis: who},
            device_id_type=MESH,
        )

    right, left = lax.rem(t + 1, T), lax.rem(t + T - 1, T)
    far = lax.rem(t + 2, T)

    def tp_copy(kind, src, dst, d):
        return remote(src, dst, tsend.at[kind, d], trecv.at[kind, d], "tp", lax.rem(t + d, T))

    def tp_wait(kind, ref, d):
        remote(ref, ref, tsend.at[kind, d], trecv.at[kind, d], "tp", right).wait_recv()

    def half(unit, block, h):
        if unit < 4:
            ref = wg if unit < 2 else wu
            n = ref.shape[1] // 4
            return ref.at[block, pl.ds((unit % 2) * 2 * n + h * n, n), :]
        n = hidden // 2
        return wd.at[unit - 4, block, pl.ds(h * n, n), :]

    def ring(unit, block, h, to_right, idx):
        ref = half(unit, block, h)
        return remote(
            ref, ref, wsend.at[unit, idx], wrecv.at[unit, idx], "tp", right if to_right else left
        )

    def direct_half(unit, h):
        ring(unit, t, h, True, 2 * h).start()
        ring(unit, t, 1 - h, False, 2 * (1 - h) + 1).start()

    def direct(unit):
        if unit >= 4:
            for i in range(per_chunk):
                loads[3 + (unit - 4) * per_chunk + i].wait()
        direct_half(unit, 0)
        direct_half(unit, 1)

    def direct_wait(unit, h, from_left):
        ring(unit, left if from_left else right, h, True, 2 * h + (0 if from_left else 1)).wait_recv()

    def relay(unit):
        direct_wait(unit, 0, True)
        ring(unit, left, 0, True, 4).start()
        direct_wait(unit, 1, False)
        ring(unit, right, 1, False, 5).start()

    def near_wait(unit):
        direct_wait(unit, 1, True)
        direct_wait(unit, 0, False)

    def far_wait(unit):
        ring(unit, far, 0, True, 4).wait_recv()
        ring(unit, far, 1, True, 5).wait_recv()

    per = ow.shape[1] // 8

    def piece(block, at_x, at_z, at_core, h=None, side=None):
        first = (at_x * 4 + at_z * 2 + at_core) * per
        if h is None:
            return ow.at[block, pl.ds(first, per), :]
        n = per // 2
        if side is None:
            return ow.at[block, pl.ds(first + h * n, n), :]
        return ow.at[block, pl.ds(first + h * n, n), pl.ds(side * (D // 2), D // 2)]

    def from_block(d):
        return lax.rem(t + T - d, T)

    def share(kind, d, ref, who):
        return remote(ref, ref, osend.at[kind, d], orecv.at[kind, d], "sp", who)

    sends = []

    def go(copy):
        copy.start()
        sends.append(copy)

    for i, src in enumerate((cv, cg)):
        go(
            remote(
                src.at[pl.ds(rows - TAPS_PAD, TAPS_PAD), :],
                halo.at[i],
                hsend.at[i],
                hrecv.at[i],
                "sp",
                lax.rem(s + 1, S),
            )
        )
    loads[0].wait()
    for d in range(1, T):
        mine = piece(t, xp, zp, core)
        go(tp_copy(3, mine, mine, d))
    for d in range(1, T):
        go(tp_copy(0, res.at[pl.ds(lax.rem(t + d, T) * Q, Q), :], res_r.at[t], d))
        go(tp_copy(1, mg, mg_r.at[t], d))
    res_r[t] = res[pl.ds(t * Q, Q), :]
    mg_r[t] = mg[...]

    for i in range(2):
        remote(halo.at[i], halo.at[i], hsend.at[i], hrecv.at[i], "tp", right).wait_recv()
    first = jnp.where(s == 0, 0.0, 1.0).astype(F32)
    gated[:TAPS_PAD, :] = halo[0].astype(F32) * sigmoid(halo[1].astype(F32)) * first

    conv_rows(0)
    stats[t] = st[...].T[:8]
    for d in range(1, T):
        go(tp_copy(2, stats.at[t], stats.at[t], d))

    loads[1].wait()
    direct_half(0, 0)

    for d in range(1, T):
        tp_wait(2, stats.at[from_block(d)], d)
    whole = stats[0]
    for b in range(1, T):
        whole = whole + stats[b]
    whole = jnp.concatenate([whole, jnp.zeros((120, rows), F32)], axis=0).T
    mean = whole[:, 0:1] / (chans * T)
    var = whole[:, 1:2] / (chans * T) - mean * mean
    wide = lax.broadcasted_iota(jnp.int32, (rows, 128), 1)
    mv[...] = jnp.where(wide == 0, mean, lax.rsqrt(var + EPS))

    def activate(q, dst):
        at = pl.ds(pl.multiple_of(q * Q, Q), Q)
        stat = mv[at, :]
        normal = (conv[at, :] - stat[:, 0:1]) * stat[:, 1:2] * gain[...] + shift[...]
        dst[...] = (normal * sigmoid(normal)).astype(BF)

    for d in (2, 1, 3):
        activate(lax.rem(t + d, T), act_s.at[d])
        go(tp_copy(4, act_s.at[d], act_r.at[t], d))
    activate(t, act_r.at[t])

    for d in range(1, T):
        b = from_block(d)
        tp_wait(3, piece(b, xp, zp, core), d)
        go(share(0, d, piece(b, xp, zp, core, 0), x_right))
        go(share(1, d, piece(b, xp, zp, core, 1), x_left))
        go(share(2, d, piece(b, xp, zp, core, 0), z_right))
        go(share(3, d, piece(b, xp, zp, core, 1), z_left))
        go(share(8, d, piece(b, xp, zp, core), other))
    direct_half(0, 1)
    direct(1)
    for d in range(1, T):
        b = from_block(d)
        for h in range(2):
            share(h, d, piece(b, 1 - xp, zp, core, h), other).wait_recv()
            share(2 + h, d, piece(b, xp, 1 - zp, core, h), other).wait_recv()
        go(share(4, d, piece(b, xp, 1 - zp, core, 0, 0), x_right))
        go(share(5, d, piece(b, xp, 1 - zp, core, 0, 1), x_left))
        go(share(6, d, piece(b, 1 - xp, zp, core, 1, 0), z_right))
        go(share(7, d, piece(b, 1 - xp, zp, core, 1, 1), z_left))
        go(share(9, d, piece(b, 1 - xp, zp, core), other))
        go(share(10, d, piece(b, xp, 1 - zp, core), other))
    loads[2].wait()
    direct(2)
    for d in range(1, T):
        b = from_block(d)
        for side in range(2):
            share(4 + side, d, piece(b, 1 - xp, 1 - zp, core, 0, side), other).wait_recv()
            share(6 + side, d, piece(b, 1 - xp, 1 - zp, core, 1, side), other).wait_recv()
        go(share(11, d, piece(b, 1 - xp, 1 - zp, core), other))

    for d in range(1, T):
        b = from_block(d)
        tp_wait(0, res_r.at[b], d)
        tp_wait(1, mg_r.at[b], d)
        tp_wait(4, act_r.at[b], d)
    for d in range(1, T):
        for i in range(4):
            at_x = xp if i % 2 == 0 else 1 - xp
            at_z = zp if i < 2 else 1 - zp
            share(8 + i, d, piece(from_block(d), at_x, at_z, 1 - core), other).wait_recv()

    square = jnp.zeros((Q, 1), F32)
    for c in range(T):
        cols = pl.ds(c * feats, feats)
        mixed = jnp.zeros((Q, feats), F32)
        for b in range(T):
            term = jnp.dot(act_r[b], ow[b, :, cols], preferred_element_type=F32)
            mixed = mixed + term.astype(BF).astype(F32)
        middle = (res_r[c].astype(F32) + mixed).astype(BF)
        mid[:, cols] = middle
        middle = middle.astype(F32)
        square = square + jnp.sum(middle * middle, axis=1, keepdims=True)
    scale = lax.rsqrt(square / D + EPS)
    for c in range(T):
        cols = pl.ds(c * feats, feats)
        normed = (mid[:, cols].astype(F32) * scale * mg_r[c]).astype(BF)
        sent = jnp.dot(send_matrix, normed, preferred_element_type=F32)
        og[:, :, cols] = sent.reshape(S, cap, feats).astype(BF)
    rc[s] = og[s]

    def sp_exchange(src, dst, send, recv):
        def one(k):
            peer = lax.rem(s + k, S)
            remote(src.at[peer], dst.at[s], send, recv, "sp", peer).start()

        one(S // 2)

        @pl.loop(1, S // 2)
        def _(i):
            one(S // 2 - i)
            one(S // 2 + i)

    def sp_wait(ref, send, recv):
        many = ref.at[pl.ds(0, S - 1)]
        return remote(many, many, send, recv, "tp", right)

    sp_exchange(og, rc, ssend.at[chunks], srecv.at[chunks])

    relay(0)
    relay(1)
    direct(3)
    direct(4)
    relay(2)
    relay(4)
    relay(3)
    direct(5)
    direct(6)
    for unit in range(4):
        near_wait(unit)
    far_wait(0)
    far_wait(1)
    sp_wait(rc, ssend.at[chunks], srecv.at[chunks]).wait_recv()
    for c in range(T):
        cols = pl.ds(c * feats, feats)
        xb[:, cols] = rc[:, :, cols].astype(F32).reshape(slots, feats).astype(BF)

    def expert(b):
        g = jnp.dot(xb[...], wg[b], preferred_element_type=F32)
        u = jnp.dot(xb[...], wu[b], preferred_element_type=F32)
        hid[b] = (g * sigmoid(g) * u).astype(BF)

    @pl.loop(0, T - 1)
    def _(i):
        expert(lax.rem(t + T - 1 + i, T))

    far_wait(2)
    far_wait(3)
    expert(far)

    for c in range(chunks):
        near_wait(4 + c)
        far_wait(4 + c)

        @pl.loop(0, 2)
        def _(r, c=c):
            n = slots // 2
            at = pl.ds(pl.multiple_of(r * n, n), n)
            total = jnp.zeros((n, width), F32)
            for b in range(T):
                term = jnp.dot(hid[b, at, :], wd[c, b], preferred_element_type=F32)
                total = total + term.astype(BF).astype(F32)
            ys[c, pl.ds(r * (S // 2), S // 2)] = total.reshape(S // 2, cap, width).astype(BF)

        yr[c, s] = ys[c, s]
        sp_exchange(ys.at[c], yr.at[c], ssend.at[c], srecv.at[c])
        if c + 1 < chunks:
            relay(5 + c)
        if c + 3 < chunks:
            direct(7 + c)

    my_rows = pl.ds(pl.multiple_of(t * Q, Q), Q)
    for c in range(chunks):
        sp_wait(yr.at[c], ssend.at[c], srecv.at[c]).wait_recv()
        back = yr[c].astype(F32).reshape(slots, width).astype(BF)
        picked = [jnp.dot(place[k], back, preferred_element_type=F32) for k in range(2)]
        added = gates[0] * picked[0] + gates[1] * picked[1]
        cols = pl.ds((c // blocks_by) * strip, strip)
        for i in range(per_chunk):
            block, at = columns(c, i)
            middle = mid[:, pl.ds(at, strip)].astype(F32)
            fin[c, i] = (middle + added[:, i * strip : (i + 1) * strip]).astype(BF)

            @pl.when(t != block)
            def _(c=c, i=i, block=block, cols=cols):
                remote(
                    fin.at[c, i], out.at[my_rows, cols], fsend.at[c, i], frecv.at[c, t], "tp", block
                ).start()

            @pl.when(t == block)
            def _(c=c, i=i, cols=cols):
                out[my_rows, cols] = fin[c, i]

    for c in range(chunks):
        sp_wait(ys.at[c], ssend.at[c], srecv.at[c]).wait_send()
    sp_wait(og, ssend.at[chunks], srecv.at[chunks]).wait_send()
    for copy in sends:
        copy.wait_send()
    for unit in range(4 + chunks):
        for idx in range(4):
            ring(unit, t, idx // 2, True, idx).wait_send()
        ring(unit, left, 0, True, 4).wait_send()
        ring(unit, right, 1, True, 5).wait_send()
    for c in range(chunks):
        for i in range(per_chunk):
            block = columns(c, i)[0]

            @pl.when(t != block)
            def _(c=c, i=i, block=block):
                remote(fin.at[c, i], fin.at[c, i], fsend.at[c, i], frecv.at[c, block], "tp", block).wait_send()

        cols = pl.ds((c // blocks_by) * strip, strip)
        mine = t // per_chunk == c % blocks_by

        @pl.when(mine)
        def _(c=c, cols=cols):
            for d in range(1, T):
                src = lax.rem(t + d, T)
                theirs = out.at[pl.ds(src * Q, Q), cols]
                remote(theirs, theirs, fsend.at[c, 0], frecv.at[c, src], "tp", src).wait_recv()


def shards(
    conv_value,
    conv_gate,
    conv_weight,
    conv_gain,
    conv_shift,
    out_weight,
    residual,
    mix_gain,
    expert_ids,
    group_weight,
    score_gap,
    w_gate,
    w_up,
    w_down,
):
    S, T = lax.axis_size("sp"), lax.axis_size("tp")
    rows, chans = conv_value.shape
    feats = residual.shape[1]
    D = feats * T
    Q = rows // T
    cap = 4 * Q // S
    slots = S * cap
    hidden = w_gate.shape[2]
    vm = pl.BlockSpec(memory_space=pltpu.VMEM)
    hbm = pl.BlockSpec(memory_space=pl.ANY)
    dma = pltpu.SemaphoreType.DMA
    return pl.pallas_call(
        functools.partial(kernel, S, T),
        name="layer",
        out_shape=jax.ShapeDtypeStruct((rows, feats), BF),
        in_specs=[vm] * 5 + [hbm] + [vm] * 5 + [hbm] * 3,
        out_specs=vm,
        scratch_shapes=[
            pltpu.VMEM((T, chans, D), BF),
            pltpu.VMEM((T, D, hidden), BF),
            pltpu.VMEM((T, D, hidden), BF),
            pltpu.VMEM((CHUNKS, T, hidden, D // CHUNKS), BF),
            pltpu.VMEM((2, TAPS_PAD, chans), BF),
            pltpu.VMEM((rows + TAPS_PAD, chans), F32),
            pltpu.VMEM((rows, chans), F32),
            pltpu.VMEM((rows, 128), F32),
            pltpu.VMEM((T, 8, rows), F32),
            pltpu.VMEM((rows, 128), F32),
            pltpu.VMEM((T, Q, chans), BF),
            pltpu.VMEM((T, Q, chans), BF),
            pltpu.VMEM((T, Q, feats), BF),
            pltpu.VMEM((T, 1, feats), F32),
            pltpu.VMEM((Q, D), BF),
            pltpu.VMEM((2, Q, slots), BF),
            pltpu.VMEM((S, cap, D), BF),
            pltpu.VMEM((S, cap, D), BF),
            pltpu.VMEM((slots, D), BF),
            pltpu.VMEM((T, slots, hidden), BF),
            pltpu.VMEM((CHUNKS, S, cap, D // CHUNKS), BF),
            pltpu.VMEM((CHUNKS, S, cap, D // CHUNKS), BF),
            pltpu.VMEM((CHUNKS, D // CHUNKS // 128, Q, 128), BF),
            dma((3 + D // 128,)),
            dma((2,)),
            dma((2,)),
            dma((5, T)),
            dma((5, T)),
            dma((12, T)),
            dma((12, T)),
            dma((4 + CHUNKS, 6)),
            dma((4 + CHUNKS, 6)),
            dma((CHUNKS + 1,)),
            dma((CHUNKS + 1,)),
            dma((CHUNKS, 2)),
            dma((CHUNKS, T)),
        ],
        compiler_params=pltpu.CompilerParams(
            collective_id=0, has_side_effects=True, vmem_limit_bytes=60 * 1024 * 1024
        ),
    )(
        conv_value,
        conv_gate,
        conv_weight,
        conv_gain.reshape(1, -1),
        conv_shift.reshape(1, -1),
        out_weight,
        residual,
        mix_gain.reshape(1, -1),
        expert_ids.T,
        group_weight.reshape(1, -1),
        score_gap.reshape(1, -1),
        w_gate,
        w_up,
        w_down,
    )


def solution(mesh):
    return jax.shard_map(
        shards,
        mesh=mesh,
        in_specs=(
            P("sp", "tp"),
            P("sp", "tp"),
            P(None, "tp"),
            P("tp"),
            P("tp"),
            P("tp", None),
            P("sp", "tp"),
            P("tp"),
            P("sp", None),
            P("sp"),
            P("sp"),
            P("sp", None, "tp"),
            P("sp", None, "tp"),
            P("sp", "tp", None),
        ),
        out_specs=P("sp", "tp"),
        check_vma=False,
    )
```

```python
import functools

import jax
import jax.numpy as jnp
from jax import lax
from jax.experimental import pallas as pl
from jax.experimental.pallas import tpu as pltpu
from jax.sharding import PartitionSpec as P

MESH = pl.DeviceIdType.MESH
BF = jnp.bfloat16
F32 = jnp.float32
EPS = 1e-06
TAPS_PAD = 32
CHUNK = 64
CHUNKS = 8
XS = 4
CORES = 2


def sigmoid(v):
    return jax.nn.sigmoid(v)


def kernel(
    S,
    T,
    cv_in,
    cg_in,
    cw_in,
    gain_in,
    shift_in,
    ow_hbm,
    res_in,
    mg_in,
    ids_in,
    gw_in,
    gap_in,
    wg_hbm,
    wu_hbm,
    wd_hbm,
    out,
    ow,
    wg,
    wu,
    wd,
    halo,
    gated,
    conv,
    st,
    stats,
    mv,
    act_s,
    act_r,
    res_r,
    mg_r,
    mid,
    place,
    og,
    rc,
    xb,
    hid,
    ys,
    yr,
    fin,
    loc,
    hsend,
    hrecv,
    tsend,
    trecv,
    osend,
    orecv,
    wsend,
    wrecv,
    ssend,
    srecv,
    fsend,
    frecv,
    cv,
    cg,
    cw,
    gain,
    shift,
    res,
    mg,
    ids,
    gw,
    gap,
    opsem,
):
    t = lax.axis_index("tp")
    s = lax.axis_index("sp")
    rows, chans = cv.shape
    taps = cw.shape[0]
    Q = rows // T
    feats = res.shape[1]
    D = feats * T
    cap = og.shape[1]
    hidden = wg.shape[2]
    chunks = ys.shape[0]
    width = D // chunks
    per_chunk = width // 128
    blocks_by = T // per_chunk
    slots = S * cap
    strip = 128
    core = lax.rem(s, CORES)
    x = lax.rem(s // CORES, XS)
    base = s - core - x * CORES
    depth = S // (XS * CORES)
    z = base // (XS * CORES)
    zp = lax.rem(z, 2)
    z_right = lax.rem(z + 1, depth) * (XS * CORES) + x * CORES + core
    z_left = lax.rem(z + depth - 1, depth) * (XS * CORES) + x * CORES + core
    other = s + 1 - 2 * core

    barrier = pltpu.get_barrier_semaphore()

    @pl.loop(1, S)
    def _(k):
        pl.semaphore_signal(
            barrier, inc=1, device_id={"sp": lax.rem(s + k, S)}, device_id_type=MESH
        )

    for d in range(1, T):
        pl.semaphore_signal(
            barrier, inc=1, device_id={"tp": lax.rem(t + d, T)}, device_id_type=MESH
        )
    loads = [pltpu.make_async_copy(ow_hbm, ow.at[t], loc.at[0])]
    operands = [
        pltpu.make_async_copy(src, dst, opsem.at[i])
        for i, (src, dst) in enumerate(
            (
                (cv_in, cv),
                (cg_in, cg),
                (mg_in, mg),
                (cw_in, cw),
                (gain_in, gain),
                (shift_in, shift),
                (ids_in, ids),
                (gw_in, gw),
                (gap_in, gap),
                (res_in, res),
            )
        )
    ]
    loads[0].start()
    for load in operands:
        load.start()
    loads.append(pltpu.make_async_copy(wg_hbm.at[0], wg.at[t], loc.at[1]))
    loads.append(pltpu.make_async_copy(wu_hbm.at[0], wu.at[t], loc.at[2]))

    def columns(c, i):
        block = (c % blocks_by) * per_chunk + i
        return block, block * feats + (c // blocks_by) * strip

    for c in range(chunks):
        for i in range(per_chunk):
            loads.append(
                pltpu.make_async_copy(
                    wd_hbm.at[0, :, pl.ds(columns(c, i)[1], strip)],
                    wd.at[c, t, :, pl.ds(i * strip, strip)],
                    loc.at[3 + c * per_chunk + i],
                )
            )
    for load in loads[1:]:
        load.start()

    pl.semaphore_wait(barrier, S - 1 + T - 1)
    for load in operands:
        load.wait()

    def remote(src, dst, send, recv, axis, who):
        return pltpu.make_async_remote_copy(
            src_ref=src,
            dst_ref=dst,
            send_sem=send,
            recv_sem=recv,
            device_id={axis: who},
            device_id_type=MESH,
        )

    right, left = lax.rem(t + 1, T), lax.rem(t + T - 1, T)
    far = lax.rem(t + 2, T)

    def tp_copy(kind, src, dst, d):
        return remote(src, dst, tsend.at[kind, d], trecv.at[kind, d], "tp", lax.rem(t + d, T))

    def tp_wait(kind, ref, d):
        remote(ref, ref, tsend.at[kind, d], trecv.at[kind, d], "tp", right).wait_recv()

    def half(unit, block, h):
        if unit < 4:
            ref = wg if unit < 2 else wu
            n = ref.shape[1] // 4
            return ref.at[block, pl.ds((unit % 2) * 2 * n + h * n, n), :]
        n = hidden // 2
        return wd.at[unit - 4, block, pl.ds(h * n, n), :]

    def ring(unit, block, h, to_right, idx):
        ref = half(unit, block, h)
        return remote(
            ref, ref, wsend.at[unit, idx], wrecv.at[unit, idx], "tp", right if to_right else left
        )

    def direct_half(unit, h):
        ring(unit, t, h, True, 2 * h).start()
        ring(unit, t, 1 - h, False, 2 * (1 - h) + 1).start()

    def direct(unit):
        if unit >= 4:
            for i in range(per_chunk):
                loads[3 + (unit - 4) * per_chunk + i].wait()
        direct_half(unit, 0)
        direct_half(unit, 1)

    def direct_wait(unit, h, from_left):
        ring(unit, left if from_left else right, h, True, 2 * h + (0 if from_left else 1)).wait_recv()

    def relay(unit):
        direct_wait(unit, 0, True)
        ring(unit, left, 0, True, 4).start()
        direct_wait(unit, 1, False)
        ring(unit, right, 1, False, 5).start()

    def near_wait(unit):
        direct_wait(unit, 1, True)
        direct_wait(unit, 0, False)

    def far_wait(unit):
        ring(unit, far, 0, True, 4).wait_recv()
        ring(unit, far, 1, True, 5).wait_recv()

    per = ow.shape[1] // (XS * 2 * CORES)

    def piece(block, at_x, at_z, at_core, h=None):
        rows_at = pl.ds(((at_x * 2 + at_z) * CORES + at_core) * per, per)
        if h is None:
            return ow.at[block, rows_at, :]
        return ow.at[block, rows_at, pl.ds(h * (D // 2), D // 2)]

    def x_back(r):
        return lax.rem(x + XS - r, XS)

    def from_block(d):
        return lax.rem(t + T - d, T)

    def share(kind, d, ref, who):
        return remote(ref, ref, osend.at[kind, d], orecv.at[kind, d], "sp", who)

    sends = []

    def go(copy):
        copy.start()
        sends.append(copy)

    for i, src in enumerate((cv, cg)):
        go(
            remote(
                src.at[pl.ds(rows - TAPS_PAD, TAPS_PAD), :],
                halo.at[i],
                hsend.at[i],
                hrecv.at[i],
                "sp",
                lax.rem(s + 1, S),
            )
        )
    loads[0].wait()
    for d in (1, 3, 2):
        mine = piece(t, x, zp, core)
        go(tp_copy(3, mine, mine, d))
    for d in range(1, T):
        go(tp_copy(1, mg, mg_r.at[t], d))
    res_r[t] = res[pl.ds(t * Q, Q), :]
    mg_r[t] = mg[...]

    gated[TAPS_PAD:, :] = cv[...].astype(F32) * sigmoid(cg[...].astype(F32))
    lane = lax.broadcasted_iota(jnp.int32, (CHUNK, 128), 1)

    def conv_rows(r):
        base = r * CHUNK if isinstance(r, int) else pl.multiple_of(r * CHUNK, CHUNK)
        span = CHUNK + TAPS_PAD
        window = gated[pl.ds(base, span), :]
        total = jnp.zeros((CHUNK, chans), F32)
        lead = TAPS_PAD - (taps - 1)
        for phase in range(8):
            turned = pltpu.roll(window, span - phase, 0) if phase else window
            for j in range(taps):
                if (lead + j) % 8 == phase:
                    at = lead + j - phase
                    total = total + cw[j : j + 1, :] * turned[at : at + CHUNK]
        conv[pl.ds(base, CHUNK), :] = total
        ssum = jnp.sum(total, axis=1, keepdims=True)
        ssq = jnp.sum(total * total, axis=1, keepdims=True)
        st[pl.ds(base, CHUNK), :] = jnp.where(lane == 0, ssum, jnp.where(lane == 1, ssq, 0.0))

    @pl.loop(1, rows // CHUNK)
    def _(r):
        conv_rows(r)

    here = pl.ds(pl.multiple_of(t * Q, Q), Q)
    E = S
    expert_iota = lax.broadcasted_iota(jnp.int32, (E, Q), 0)
    id_rows = [ids[k : k + 1, here] for k in range(2)]
    hits = [(expert_iota == id_rows[k]).astype(F32) for k in range(2)]
    upper = (
        lax.broadcasted_iota(jnp.int32, (Q, Q), 0) < lax.broadcasted_iota(jnp.int32, (Q, Q), 1)
    ).astype(BF)
    before = jnp.dot((hits[0] + hits[1]).astype(BF), upper, preferred_element_type=F32)
    slot_rows = [
        id_rows[k].astype(F32) * cap + jnp.sum(before * hits[k], axis=0, keepdims=True)
        for k in range(2)
    ]
    slot_iota = lax.broadcasted_iota(jnp.int32, (slots, Q), 0).astype(F32)
    send_matrix = jnp.where(
        (slot_iota == slot_rows[0]) | (slot_iota == slot_rows[1]), 1.0, 0.0
    ).astype(BF)
    weight = gw[:, here]
    gate_rows = [weight * sigmoid(gap[:, here]), weight * sigmoid(-gap[:, here])]
    table = jnp.concatenate(slot_rows + gate_rows + [jnp.zeros((Q - 4, Q), F32)], axis=0).T
    lane_iota = lax.broadcasted_iota(jnp.int32, (Q, slots), 1).astype(F32)
    for k in range(2):
        place[k] = jnp.where(lane_iota == table[:, k : k + 1], 1.0, 0.0).astype(BF)
    gates = [table[:, 2 + k : 3 + k] for k in range(2)]

    for i in range(2):
        remote(halo.at[i], halo.at[i], hsend.at[i], hrecv.at[i], "tp", right).wait_recv()
    first = jnp.where(s == 0, 0.0, 1.0).astype(F32)
    gated[:TAPS_PAD, :] = halo[0].astype(F32) * sigmoid(halo[1].astype(F32)) * first

    conv_rows(0)
    stats[t] = st[...].T[:8]
    for d in range(1, T):
        go(tp_copy(2, stats.at[t], stats.at[t], d))

    loads[1].wait()
    direct_half(0, 0)

    def to_z(d, r):
        block, at_x = from_block(d), x_back(r)
        go(share(3 + 2 * r, d, piece(block, at_x, zp, core, 0), z_right))
        go(share(4 + 2 * r, d, piece(block, at_x, zp, core, 1), z_left))
        go(share(11 + 2 * r, d, piece(block, at_x, zp, core), other))

    def pass_on(d):
        mine = piece(from_block(d), x, zp, core)
        tp_wait(3, mine, d)
        for r in range(1, XS):
            go(share(r - 1, d, mine, base + lax.rem(x + r, XS) * CORES + core))
        to_z(d, 0)

    pass_on(1)
    pass_on(3)

    for d in range(1, T):
        tp_wait(2, stats.at[from_block(d)], d)
    whole = stats[0]
    for b in range(1, T):
        whole = whole + stats[b]
    whole = jnp.concatenate([whole, jnp.zeros((120, rows), F32)], axis=0).T
    mean = whole[:, 0:1] / (chans * T)
    var = whole[:, 1:2] / (chans * T) - mean * mean
    wide = lax.broadcasted_iota(jnp.int32, (rows, 128), 1)
    mv[...] = jnp.where(wide == 0, mean, lax.rsqrt(var + EPS))

    def activate(q, dst):
        at = pl.ds(pl.multiple_of(q * Q, Q), Q)
        stat = mv[at, :]
        normal = (conv[at, :] - stat[:, 0:1]) * stat[:, 1:2] * gain[...] + shift[...]
        dst[...] = (normal * sigmoid(normal)).astype(BF)

    for d in (2, 1, 3):
        activate(lax.rem(t + d, T), act_s.at[d])
        go(tp_copy(4, act_s.at[d], act_r.at[t], d))
    activate(t, act_r.at[t])
    for d in range(1, T):
        go(tp_copy(0, res.at[pl.ds(lax.rem(t + d, T) * Q, Q), :], res_r.at[t], d))

    pass_on(2)
    direct_half(0, 1)
    direct(1)
    for r in (1, 3, 2):
        for d in (1, 3, 2):
            share(r - 1, d, piece(from_block(d), x_back(r), zp, core), other).wait_recv()
            to_z(d, r)
    loads[2].wait()
    direct(2)
    for r in (0, 1, 3, 2):
        for d in (1, 3, 2):
            block, at_x = from_block(d), x_back(r)
            for h in range(2):
                share(3 + 2 * r + h, d, piece(block, at_x, 1 - zp, core, h), other).wait_recv()
            go(share(12 + 2 * r, d, piece(block, at_x, 1 - zp, core), other))

    for d in range(1, T):
        b = from_block(d)
        tp_wait(0, res_r.at[b], d)
        tp_wait(1, mg_r.at[b], d)
        tp_wait(4, act_r.at[b], d)
    for d in range(1, T):
        for r in range(XS):
            for far_z in range(2):
                at_z = 1 - zp if far_z else zp
                share(
                    11 + 2 * r + far_z, d, piece(from_block(d), x_back(r), at_z, 1 - core), other
                ).wait_recv()

    square = jnp.zeros((Q, 1), F32)
    for c in range(T):
        cols = pl.ds(c * feats, feats)
        mixed = jnp.zeros((Q, feats), F32)
        for b in range(T):
            term = jnp.dot(act_r[b], ow[b, :, cols], preferred_element_type=F32)
            mixed = mixed + term.astype(BF).astype(F32)
        middle = (res_r[c].astype(F32) + mixed).astype(BF)
        mid[:, cols] = middle
        middle = middle.astype(F32)
        square = square + jnp.sum(middle * middle, axis=1, keepdims=True)
    scale = lax.rsqrt(square / D + EPS)
    for c in range(T):
        cols = pl.ds(c * feats, feats)
        normed = (mid[:, cols].astype(F32) * scale * mg_r[c]).astype(BF)
        sent = jnp.dot(send_matrix, normed, preferred_element_type=F32)
        og[:, :, cols] = sent.reshape(S, cap, feats).astype(BF)
    rc[s] = og[s]

    def sp_exchange(src, dst, send, recv):
        def one(k):
            peer = lax.rem(s + k, S)
            remote(src.at[peer], dst.at[s], send, recv, "sp", peer).start()

        one(S // 2)

        @pl.loop(1, S // 2)
        def _(i):
            one(S // 2 - i)
            one(S // 2 + i)

    def sp_wait(ref, send, recv):
        many = ref.at[pl.ds(0, S - 1)]
        return remote(many, many, send, recv, "tp", right)

    sp_exchange(og, rc, ssend.at[chunks], srecv.at[chunks])

    relay(0)
    relay(1)
    direct(3)
    direct(4)
    relay(2)
    relay(4)
    relay(3)
    direct(5)
    direct(6)
    for unit in range(4):
        near_wait(unit)
    far_wait(0)
    far_wait(1)
    sp_wait(rc, ssend.at[chunks], srecv.at[chunks]).wait_recv()
    for c in range(T):
        cols = pl.ds(c * feats, feats)
        xb[:, cols] = rc[:, :, cols].astype(F32).reshape(slots, feats).astype(BF)

    def expert(b):
        g = jnp.dot(xb[...], wg[b], preferred_element_type=F32)
        u = jnp.dot(xb[...], wu[b], preferred_element_type=F32)
        hid[b] = (g * sigmoid(g) * u).astype(BF)

    @pl.loop(0, T - 1)
    def _(i):
        expert(lax.rem(t + T - 1 + i, T))

    far_wait(2)
    far_wait(3)
    expert(far)

    for c in range(chunks):
        near_wait(4 + c)
        far_wait(4 + c)

        @pl.loop(0, 2)
        def _(r, c=c):
            n = slots // 2
            at = pl.ds(pl.multiple_of(r * n, n), n)
            total = jnp.zeros((n, width), F32)
            for b in range(T):
                term = jnp.dot(hid[b, at, :], wd[c, b], preferred_element_type=F32)
                total = total + term.astype(BF).astype(F32)
            ys[c, pl.ds(r * (S // 2), S // 2)] = total.reshape(S // 2, cap, width).astype(BF)

        yr[c, s] = ys[c, s]
        sp_exchange(ys.at[c], yr.at[c], ssend.at[c], srecv.at[c])
        if c + 1 < chunks:
            relay(5 + c)
        if c + 3 < chunks:
            direct(7 + c)

    my_rows = pl.ds(pl.multiple_of(t * Q, Q), Q)
    for c in range(chunks):
        sp_wait(yr.at[c], ssend.at[c], srecv.at[c]).wait_recv()
        back = yr[c].astype(F32).reshape(slots, width).astype(BF)
        picked = [jnp.dot(place[k], back, preferred_element_type=F32) for k in range(2)]
        added = gates[0] * picked[0] + gates[1] * picked[1]
        cols = pl.ds((c // blocks_by) * strip, strip)
        for i in range(per_chunk):
            block, at = columns(c, i)
            middle = mid[:, pl.ds(at, strip)].astype(F32)
            fin[c, i] = (middle + added[:, i * strip : (i + 1) * strip]).astype(BF)

            @pl.when(t != block)
            def _(c=c, i=i, block=block, cols=cols):
                remote(
                    fin.at[c, i], out.at[my_rows, cols], fsend.at[c, i], frecv.at[c, t], "tp", block
                ).start()

            @pl.when(t == block)
            def _(c=c, i=i, cols=cols):
                out[my_rows, cols] = fin[c, i]

    for c in range(chunks):
        sp_wait(ys.at[c], ssend.at[c], srecv.at[c]).wait_send()
    sp_wait(og, ssend.at[chunks], srecv.at[chunks]).wait_send()
    for copy in sends:
        copy.wait_send()
    for unit in range(4 + chunks):
        for idx in range(4):
            ring(unit, t, idx // 2, True, idx).wait_send()
        ring(unit, left, 0, True, 4).wait_send()
        ring(unit, right, 1, True, 5).wait_send()
    for c in range(chunks):
        for i in range(per_chunk):
            block = columns(c, i)[0]

            @pl.when(t != block)
            def _(c=c, i=i, block=block):
                remote(fin.at[c, i], fin.at[c, i], fsend.at[c, i], frecv.at[c, block], "tp", block).wait_send()

        cols = pl.ds((c // blocks_by) * strip, strip)
        mine = t // per_chunk == c % blocks_by

        @pl.when(mine)
        def _(c=c, cols=cols):
            for d in range(1, T):
                src = lax.rem(t + d, T)
                theirs = out.at[pl.ds(src * Q, Q), cols]
                remote(theirs, theirs, fsend.at[c, 0], frecv.at[c, src], "tp", src).wait_recv()


def shards(
    conv_value,
    conv_gate,
    conv_weight,
    conv_gain,
    conv_shift,
    out_weight,
    residual,
    mix_gain,
    expert_ids,
    group_weight,
    score_gap,
    w_gate,
    w_up,
    w_down,
):
    S, T = lax.axis_size("sp"), lax.axis_size("tp")
    rows, chans = conv_value.shape
    feats = residual.shape[1]
    D = feats * T
    Q = rows // T
    cap = 4 * Q // S
    slots = S * cap
    hidden = w_gate.shape[2]
    vm = pl.BlockSpec(memory_space=pltpu.VMEM)
    hbm = pl.BlockSpec(memory_space=pl.ANY)
    dma = pltpu.SemaphoreType.DMA
    return pl.pallas_call(
        functools.partial(kernel, S, T),
        name="layer",
        out_shape=jax.ShapeDtypeStruct((rows, feats), BF),
        in_specs=[hbm] * 14,
        out_specs=vm,
        scratch_shapes=[
            pltpu.VMEM((T, chans, D), BF),
            pltpu.VMEM((T, D, hidden), BF),
            pltpu.VMEM((T, D, hidden), BF),
            pltpu.VMEM((CHUNKS, T, hidden, D // CHUNKS), BF),
            pltpu.VMEM((2, TAPS_PAD, chans), BF),
            pltpu.VMEM((rows + TAPS_PAD, chans), F32),
            pltpu.VMEM((rows, chans), F32),
            pltpu.VMEM((rows, 128), F32),
            pltpu.VMEM((T, 8, rows), F32),
            pltpu.VMEM((rows, 128), F32),
            pltpu.VMEM((T, Q, chans), BF),
            pltpu.VMEM((T, Q, chans), BF),
            pltpu.VMEM((T, Q, feats), BF),
            pltpu.VMEM((T, 1, feats), F32),
            pltpu.VMEM((Q, D), BF),
            pltpu.VMEM((2, Q, slots), BF),
            pltpu.VMEM((S, cap, D), BF),
            pltpu.VMEM((S, cap, D), BF),
            pltpu.VMEM((slots, D), BF),
            pltpu.VMEM((T, slots, hidden), BF),
            pltpu.VMEM((CHUNKS, S, cap, D // CHUNKS), BF),
            pltpu.VMEM((CHUNKS, S, cap, D // CHUNKS), BF),
            pltpu.VMEM((CHUNKS, D // CHUNKS // 128, Q, 128), BF),
            dma((3 + D // 128,)),
            dma((2,)),
            dma((2,)),
            dma((5, T)),
            dma((5, T)),
            dma((19, T)),
            dma((19, T)),
            dma((4 + CHUNKS, 6)),
            dma((4 + CHUNKS, 6)),
            dma((CHUNKS + 1,)),
            dma((CHUNKS + 1,)),
            dma((CHUNKS, 2)),
            dma((CHUNKS, T)),
            pltpu.VMEM((rows, chans), BF),
            pltpu.VMEM((rows, chans), BF),
            pltpu.VMEM(conv_weight.shape, F32),
            pltpu.VMEM((1, chans), F32),
            pltpu.VMEM((1, chans), F32),
            pltpu.VMEM((rows, feats), BF),
            pltpu.VMEM((1, feats), F32),
            pltpu.VMEM((2, rows), jnp.int32),
            pltpu.VMEM((1, rows), F32),
            pltpu.VMEM((1, rows), F32),
            dma((10,)),
        ],
        compiler_params=pltpu.CompilerParams(
            collective_id=0, has_side_effects=True, vmem_limit_bytes=60 * 1024 * 1024
        ),
    )(
        conv_value,
        conv_gate,
        conv_weight,
        conv_gain.reshape(1, -1),
        conv_shift.reshape(1, -1),
        out_weight,
        residual,
        mix_gain.reshape(1, -1),
        expert_ids.T,
        group_weight.reshape(1, -1),
        score_gap.reshape(1, -1),
        w_gate,
        w_up,
        w_down,
    )


def solution(mesh):
    return jax.shard_map(
        shards,
        mesh=mesh,
        in_specs=(
            P("sp", "tp"),
            P("sp", "tp"),
            P(None, "tp"),
            P("tp"),
            P("tp"),
            P("tp", None),
            P("sp", "tp"),
            P("tp"),
            P("sp", None),
            P("sp"),
            P("sp"),
            P("sp", None, "tp"),
            P("sp", None, "tp"),
            P("sp", "tp", None),
        ),
        out_specs=P("sp", "tp"),
        check_vma=False,
    )
```
